32 devices in a mesh: sp: 4 (over z), fs: 4 (over y, x), tp: 2 (over core).
Axes of the slice: x: 2, y: 2, z: 4, core: 2. Of those that a mesh axis runs over, the one named last changes fastest.
Arguments:
- tokens: bfloat16 [4, 512, 2048], P('fs', 'sp', 'tp'), may hold values from -6 to 6
- norm_gain: float32 [2048], replicated, may hold values from 0.1 to 1.9
- conv_gate_out: bfloat16 [2048, 512], P(('sp', 'fs'), 'tp'), may hold values from -0.125 to 0.125
- conv_gate_in: bfloat16 [2048, 512], P(('sp', 'fs'), 'tp'), may hold values from -0.125 to 0.125
- conv_value: bfloat16 [2048, 512], P(('sp', 'fs'), 'tp'), may hold values from -0.125 to 0.125
- conv_taps: float32 [3, 512], P(None, 'tp'), may hold values from -3.5 to 3.5
- recv_weight: bfloat16 [2048, 512], P(('sp', 'fs'), 'tp'), may hold values from -0.125 to 0.125
- key_weight: bfloat16 [2048, 512], P(('sp', 'fs'), 'tp'), may hold values from -0.125 to 0.125
- value_weight: bfloat16 [2048, 512], P(('sp', 'fs'), 'tp'), may hold values from -0.125 to 0.125
- decay_base: float32 [512], P('tp'), may hold values from -12.5 to -3.3
- decay_down: bfloat16 [2048, 64], replicated, may hold values from -0.125 to 0.125
- decay_up: bfloat16 [64, 512], P(None, 'tp'), may hold values from -1.5 to 1.5
- decay_shift: float32 [4, 512, 8], P('fs', 'sp', 'tp'), may hold values from -0.7 to 11.5
- rate_base: float32 [512], P('tp'), may hold values from -4 to 4
- rate_down: bfloat16 [2048, 64], replicated, may hold values from -0.125 to 0.125
- rate_up: bfloat16 [64, 512], P(None, 'tp'), may hold values from -0.75 to 0.75
- head_gain: float32 [512], P('tp'), may hold values from 0.1 to 1.9
- out_conv: bfloat16 [512, 2048], P('tp', ('sp', 'fs')), may hold values from -0.1875 to 0.1875
- out_state: bfloat16 [512, 2048], P('tp', ('sp', 'fs')), may hold values from -0.1875 to 0.1875
Outputs:
- mixed_out: bfloat16 [4, 512, 2048], P('fs', ('sp', 'tp'))
The draws below stay inside these ranges and needn't reach their ends.
All inputs are finite; a program needn't handle non-finite values.
Results may differ from the reference program's by a relative error of at most 0.015.
Values may be sent and summed in bfloat16 or wider, within the bound.
A program may use at most 64 MiB of HBM per device.

```python
import jax
import jax.numpy as jnp
from jax import lax

D = 2048
CW = 512
RH = 8
HD = 64
LOW = 64
TOK_DEV = 128
RW = 512
SEQS = 4
SEQ = 512
N_TP = 2


def draw_decay_base(key, part):
    choose_key = jax.random.fold_in(key, 11)
    slow_key = jax.random.fold_in(key, 12)
    fast_key = jax.random.fold_in(key, 13)
    slow_share = 0.5
    slow_heads = jax.random.uniform(choose_key, (RH, 1), jnp.float32) < slow_share
    slow_values = jax.random.uniform(slow_key, (RH, HD), jnp.float32, -12.5, -10.5)
    fast_values = jax.random.uniform(fast_key, (RH, HD), jnp.float32, -4.3, -3.3)
    return jnp.where(slow_heads, slow_values, fast_values).reshape(RH * HD)


def draw_decay_shift(key, part):
    level_key = jax.random.fold_in(key, 21)
    spot_key = jax.random.fold_in(key, 22)
    lift_key = jax.random.fold_in(key, 23)
    blocks = SEQ // TOK_DEV
    level = jax.random.uniform(level_key, (SEQS, blocks, 1, RH), jnp.float32, -0.7, 0.7)
    level = jnp.broadcast_to(level, (SEQS, blocks, TOK_DEV, RH)).reshape(SEQS, SEQ, RH)
    spots = jax.random.randint(spot_key, (SEQS, 3), 0, SEQ)
    positions = jnp.arange(SEQ, dtype=jnp.int32)
    struck = jnp.any(positions[None, :, None] == spots[:, None, :], axis=-1)
    lift = jax.random.uniform(lift_key, (SEQS, SEQ, RH), jnp.float32, 10.5, 11.5)
    return jnp.where(struck[:, :, None], lift, level)


def block_scale(key, dims, cuts, least, high):
    loudness = 1.0
    for position, shards_of in cuts:
        heights = jax.random.uniform(jax.random.fold_in(jax.random.fold_in(key, 6), position), (shards_of,), jnp.float32, least / len(cuts), high / len(cuts))
        loudness = loudness * jnp.repeat(jnp.exp(heights), dims[position] // shards_of).reshape((-1,) + (1,) * (len(dims) - 1 - position))
    return loudness


def normal_values(own_key, shape, spread, bound, cuts=(), held_as=jnp.bfloat16):
    drawn = spread * jax.random.normal(own_key, shape, jnp.float32)
    if cuts:
        drawn = drawn * block_scale(own_key, shape, cuts, -0.22, 0.18)
    return jnp.clip(drawn, -bound, bound).astype(held_as)


def setup_inputs(seed: int = 0) -> dict:
    key_of = jax.random.split(jax.random.key(seed), 20)
    return {
        "tokens": normal_values(key_of[0], (SEQS, SEQ, D), 1.0, 6.0, ((0, 4), (1, 4), (2, 2))),
        "norm_gain": jnp.clip(1.0 + 0.18 * jax.random.normal(key_of[1], (D,), jnp.float32), 0.1, 1.9),
        "conv_gate_out": normal_values(key_of[2], (D, CW), D ** -0.5, 0.125, ((0, 16), (1, 2))),
        "conv_gate_in": normal_values(key_of[3], (D, CW), D ** -0.5, 0.125, ((0, 16), (1, 2))),
        "conv_value": normal_values(key_of[4], (D, CW), D ** -0.5, 0.125, ((0, 16), (1, 2))),
        "conv_taps": normal_values(key_of[5], (3, CW), 3 ** -0.5, 3.5, ((1, 2),), jnp.float32),
        "recv_weight": normal_values(key_of[6], (D, RW), D ** -0.5, 0.125, ((0, 16), (1, 2))),
        "key_weight": normal_values(key_of[7], (D, RW), D ** -0.5, 0.125, ((0, 16), (1, 2))),
        "value_weight": normal_values(key_of[8], (D, RW), D ** -0.5, 0.125, ((0, 16), (1, 2))),
        "decay_base": draw_decay_base(jax.random.fold_in(key_of[19], 71), 0),
        "decay_down": normal_values(key_of[10], (D, LOW), D ** -0.5, 0.125),
        "decay_up": normal_values(key_of[11], (LOW, RW), (LOW // 4) ** -0.5, 1.5, ((1, 2),)),
        "decay_shift": draw_decay_shift(jax.random.fold_in(key_of[19], 71), 0),
        "rate_base": normal_values(key_of[13], (RW,), 1.0, 4.0, ((0, 2),), jnp.float32),
        "rate_down": normal_values(key_of[14], (D, LOW), D ** -0.5, 0.125),
        "rate_up": normal_values(key_of[15], (LOW, RW), LOW ** -0.5, 0.75, ((1, 2),)),
        "head_gain": jnp.clip(1.0 + 0.18 * jax.random.normal(key_of[16], (RW,), jnp.float32), 0.1, 1.9),
        "out_conv": normal_values(key_of[17], (CW, D), (CW + RW) ** -0.5, 0.1875, ((0, 2), (1, 16))),
        "out_state": normal_values(key_of[18], (RW, D), (CW + RW) ** -0.5, 0.1875, ((0, 2), (1, 16))),
    }


RMS_EPS = 1e-05
GROUP_EPS = 0.00064
UNIT_EPS = 1e-06
HIGHEST = lax.Precision.HIGHEST

def project(normed, weight):
    return jnp.dot(normed, weight, preferred_element_type=jnp.float32).astype(jnp.bfloat16)

def recur(carried, inputs):
    keys_t, vals_t, recv_t, rate_t, decay_t = inputs
    keys_f = keys_t.astype(jnp.float32)
    vals_f = vals_t.astype(jnp.float32)
    recv_f = recv_t.astype(jnp.float32)
    unit_keys = keys_f * lax.rsqrt(lax.optimization_barrier(jnp.sum(keys_f * keys_f, axis=-1, keepdims=True)) + UNIT_EPS)
    removed = jnp.einsum('shvk,shk->shv', carried, -unit_keys, precision=HIGHEST)
    carried = carried * jnp.exp(decay_t)[:, :, None, :] + removed[..., None] * (unit_keys * rate_t)[:, :, None, :] + vals_f[..., None] * (keys_f * rate_t)[:, :, None, :]
    return (carried, jnp.einsum('shvk,shk->shv', carried, recv_f, precision=HIGHEST))

def reference(tokens, norm_gain, conv_gate_out, conv_gate_in, conv_value, conv_taps, recv_weight, key_weight, value_weight, decay_base, decay_down, decay_up, decay_shift, rate_base, rate_down, rate_up, head_gain, out_conv, out_state):
    rows_all = SEQS * SEQ
    flat = tokens.reshape(rows_all, D).astype(jnp.float32)
    normed = (flat * lax.rsqrt(lax.optimization_barrier(jnp.mean(flat * flat, axis=-1, keepdims=True)) + RMS_EPS) * norm_gain).astype(jnp.bfloat16)
    gate_out = project(normed, conv_gate_out).astype(jnp.float32).reshape(SEQS, SEQ, CW)
    gate_in = project(normed, conv_gate_in).astype(jnp.float32)
    conv_in = project(normed, conv_value).astype(jnp.float32)
    mixed_in = (gate_in * conv_in).reshape(SEQS, SEQ, CW)
    padded = jnp.pad(mixed_in, ((0, 0), (2, 0), (0, 0)))
    convolved = padded[:, 0:SEQ] * conv_taps[0] + padded[:, 1:SEQ + 1] * conv_taps[1] + padded[:, 2:SEQ + 2] * conv_taps[2]
    conv_out = (gate_out * convolved).astype(jnp.bfloat16).reshape(rows_all, CW)
    recv = project(normed, recv_weight)
    keys = project(normed, key_weight)
    vals = project(normed, value_weight)
    decay_low = jnp.tanh(jnp.dot(normed, decay_down, preferred_element_type=jnp.float32)).astype(jnp.bfloat16)
    rate_low = project(normed, rate_down)
    decay_pre = decay_base + jnp.dot(decay_low, decay_up, preferred_element_type=jnp.float32)
    log_base = -jax.nn.softplus(-decay_pre) - 0.5
    log_decay = -jnp.exp(log_base.reshape(SEQS, SEQ, RH, HD) + decay_shift[..., None])
    learn_rate = jax.nn.sigmoid(rate_base + jnp.dot(rate_low, rate_up, preferred_element_type=jnp.float32))

    def by_time(field):
        return jnp.swapaxes(field.reshape(SEQS, SEQ, RH, HD), 0, 1)
    start_state = jnp.zeros((SEQS, RH, HD, HD), jnp.float32)
    final_state, read_out = lax.scan(recur, start_state, (by_time(keys), by_time(vals), by_time(recv), by_time(learn_rate), by_time(log_decay)))
    state_read = jnp.swapaxes(read_out, 0, 1)
    centre = lax.optimization_barrier(jnp.mean(state_read, axis=-1, keepdims=True))
    centred = state_read - centre
    variance = lax.optimization_barrier(jnp.mean(centred * centred, axis=-1, keepdims=True))
    state_out = ((centred * lax.rsqrt(variance + GROUP_EPS)).reshape(rows_all, RW) * head_gain).astype(jnp.bfloat16)
    conv_block = CW // N_TP
    state_block = RW // N_TP
    total = jnp.zeros((rows_all, D), jnp.float32)
    for group in range(N_TP):
        partial_sum = jnp.dot(conv_out[:, group * conv_block:(group + 1) * conv_block], out_conv[group * conv_block:(group + 1) * conv_block], preferred_element_type=jnp.float32) + jnp.dot(state_out[:, group * state_block:(group + 1) * state_block], out_state[group * state_block:(group + 1) * state_block], preferred_element_type=jnp.float32)
        rounded = lax.optimization_barrier(partial_sum.astype(jnp.bfloat16))
        total = total + rounded.astype(jnp.float32)
    return total.astype(jnp.bfloat16).reshape(SEQS, SEQ, D)
```

```python
from functools import partial
import math

import jax
import jax.numpy as jnp
import numpy as np
from jax import lax
from jax.experimental import pallas as pl
from jax.experimental.pallas import tpu as pltpu
from jax.sharding import PartitionSpec as P

RMS_EPS = 1e-05
GROUP_EPS = 0.00064
UNIT_EPS = 1e-06
HIGHEST = lax.Precision.HIGHEST
MESH = pl.DeviceIdType.MESH


def from_behind(array, axis, by):
    size = lax.axis_size(axis)
    pairs = [(i, i + by) for i in range(size) if 0 <= i + by < size]
    return lax.ppermute(array, axis, pairs)


def carried_in(array, axis, combine, identity):
    size, index = (lax.axis_size(axis), lax.axis_index(axis))
    everything = jax.tree.map(
        lambda part, kind: lax.all_gather(part.astype(kind), axis),
        array,
        (jnp.bfloat16, jnp.bfloat16),
    )
    start = jax.tree.map(
        lambda part, zero: jnp.broadcast_to(jnp.asarray(zero, part.dtype), part.shape),
        array,
        identity,
    )

    def lap(k, before):
        reached = k < index
        new = combine(
            before, jax.tree.map(lambda part, own: part[k].astype(own.dtype), everything, array)
        )
        return jax.tree.map(lambda a, b: jnp.where(reached, a, b), new, before)

    return lax.fori_loop(0, size, lap, start)


def fold_rows(normed, totals, pieces, offset):
    return tuple(
        (
            jnp.dot(normed, pieces[member], preferred_element_type=jnp.float32)
            for member in range(len(pieces))
        )
    )


def block_step(carried, inputs):
    log_dec, remove_dir, write_dir, key_rate, receive, val_rows = inputs
    cumulative = jnp.cumsum(log_dec, axis=1)
    exclusive = cumulative - log_dec
    length = log_dec.shape[1]
    where_t = lax.broadcasted_iota(jnp.int32, (length, length), 0)
    where_s = lax.broadcasted_iota(jnp.int32, (length, length), 1)
    strict = (where_t > where_s)[None, :, :, None]
    inclusive = (where_t >= where_s)[None, :, :, None]
    damp_prior = jnp.where(
        strict, jnp.exp(jnp.minimum(exclusive[:, :, None, :] - cumulative[:, None, :, :], 0.0)), 0.0
    )
    damp_now = jnp.where(
        inclusive,
        jnp.exp(jnp.minimum(cumulative[:, :, None, :] - cumulative[:, None, :, :], 0.0)),
        0.0,
    )
    link_ab = jnp.einsum("htc,htsc,hsc->hts", remove_dir, damp_prior, write_dir, precision=HIGHEST)
    link_ak = jnp.einsum("htc,htsc,hsc->hts", remove_dir, damp_prior, key_rate, precision=HIGHEST)
    from_start = jnp.einsum(
        "hrc,htc->htr", carried, remove_dir * jnp.exp(exclusive), precision=HIGHEST
    )
    rhs_terms = from_start + jnp.einsum("hts,hsr->htr", link_ak, val_rows, precision=HIGHEST)
    unit_matrix = jnp.eye(length, dtype=jnp.float32)
    projected = lax.linalg.triangular_solve(
        unit_matrix - link_ab, rhs_terms, left_side=True, lower=True, unit_diagonal=True
    )
    read_b = jnp.einsum("htc,htsc,hsc->hts", receive, damp_now, write_dir, precision=HIGHEST)
    read_k = jnp.einsum("htc,htsc,hsc->hts", receive, damp_now, key_rate, precision=HIGHEST)
    outputs = (
        jnp.einsum("hrc,htc->htr", carried, receive * jnp.exp(cumulative), precision=HIGHEST)
        + jnp.einsum("hts,hsr->htr", read_b, projected, precision=HIGHEST)
        + jnp.einsum("hts,hsr->htr", read_k, val_rows, precision=HIGHEST)
    )
    to_end = jnp.exp(cumulative[:, -1:, :] - cumulative)
    new_state = (
        carried * jnp.exp(cumulative[:, -1, :])[:, None, :]
        + jnp.einsum("hsr,hsc->hrc", projected, write_dir * to_end, precision=HIGHEST)
        + jnp.einsum("hsr,hsc->hrc", val_rows, key_rate * to_end, precision=HIGHEST)
    )
    return (new_state, outputs)


def compose(earlier, later):
    return (
        jnp.einsum("hij,hjk->hik", earlier[0], later[0], precision=HIGHEST),
        jnp.einsum("hij,hjk->hik", earlier[1], later[0], precision=HIGHEST) + later[1],
    )


def body(
    tokens,
    norm_gain,
    conv_gate_out,
    conv_gate_in,
    conv_value,
    conv_taps,
    recv_weight,
    key_weight,
    value_weight,
    decay_base,
    decay_down,
    decay_up,
    decay_shift,
    rate_base,
    rate_down,
    rate_up,
    head_gain,
    out_conv,
    out_state,
):
    tok_count = tokens.shape[1]
    own_half = tokens.reshape(tok_count, tokens.shape[2])
    features = lax.all_gather(own_half, "tp", axis=1, tiled=True).astype(jnp.float32)
    normed = (
        features
        * lax.rsqrt(jnp.mean(features * features, axis=-1, keepdims=True) + RMS_EPS)
        * norm_gain
    ).astype(jnp.bfloat16)
    widths = (
        conv_gate_out.shape[1],
        conv_gate_in.shape[1],
        conv_value.shape[1],
        recv_weight.shape[1],
        key_weight.shape[1],
        value_weight.shape[1],
    )
    zeros_init = tuple(
        (jnp.zeros((tok_count, column_count), jnp.float32) for column_count in widths)
    )
    row_adder = partial(fold_rows, normed)
    local_go, local_gi, local_cv, local_rw, local_kw, local_vw = (
        lax.all_gather(conv_gate_out, "fs", axis=0, tiled=True),
        lax.all_gather(conv_gate_in, "fs", axis=0, tiled=True),
        lax.all_gather(conv_value, "fs", axis=0, tiled=True),
        lax.all_gather(recv_weight, "fs", axis=0, tiled=True),
        lax.all_gather(key_weight, "fs", axis=0, tiled=True),
        lax.all_gather(value_weight, "fs", axis=0, tiled=True),
    )
    projected_sums = row_adder(
        zeros_init,
        (
            lax.all_gather(local_go, "sp", axis=0, tiled=True),
            lax.all_gather(local_gi, "sp", axis=0, tiled=True),
            lax.all_gather(local_cv, "sp", axis=0, tiled=True),
            lax.all_gather(local_rw, "sp", axis=0, tiled=True),
            lax.all_gather(local_kw, "sp", axis=0, tiled=True),
            lax.all_gather(local_vw, "sp", axis=0, tiled=True),
        ),
        jnp.int32(0),
    )
    gate_out, gate_in, conv_in, recv_raw, keys_raw, vals_raw = tuple(
        (member.astype(jnp.bfloat16) for member in projected_sums)
    )
    mixed_in = gate_in.astype(jnp.float32) * conv_in.astype(jnp.float32)
    edge_rows = from_behind(mixed_in[-2:], "sp", 1)
    padded = jnp.concatenate([edge_rows, mixed_in], axis=0)
    convolved = (
        padded[0:tok_count] * conv_taps[0]
        + padded[1 : tok_count + 1] * conv_taps[1]
        + padded[2:] * conv_taps[2]
    )
    conv_out = (gate_out.astype(jnp.float32) * convolved).astype(jnp.bfloat16)
    heads_here = decay_shift.shape[2]
    head_size = recv_raw.shape[1] // heads_here
    shaped = (tok_count, heads_here, head_size)
    decay_low = jnp.tanh(jnp.dot(normed, decay_down, preferred_element_type=jnp.float32)).astype(
        jnp.bfloat16
    )
    rate_low = jnp.dot(normed, rate_down, preferred_element_type=jnp.float32).astype(jnp.bfloat16)
    decay_pre = decay_base + jnp.dot(decay_low, decay_up, preferred_element_type=jnp.float32)
    log_base = -jax.nn.softplus(-decay_pre) - 0.5
    log_decay = -jnp.exp(log_base.reshape(shaped) + decay_shift.reshape(tok_count, heads_here, 1))
    learn_rate = jax.nn.sigmoid(
        rate_base + jnp.dot(rate_low, rate_up, preferred_element_type=jnp.float32)
    ).reshape(shaped)
    keys_float = keys_raw.astype(jnp.float32).reshape(shaped)
    unit_keys = keys_float * lax.rsqrt(
        jnp.sum(keys_float * keys_float, axis=-1, keepdims=True) + UNIT_EPS
    )
    values_float = vals_raw.astype(jnp.float32).reshape(shaped)
    recv_float = recv_raw.astype(jnp.float32).reshape(shaped)
    block_len = math.gcd(tok_count, 32)
    blocks = tok_count // block_len

    def to_blocks(field):
        return field.reshape(blocks, block_len, heads_here, field.shape[2]).transpose(0, 2, 1, 3)

    val_rows = jnp.concatenate([values_float, jnp.zeros_like(values_float)], axis=2)
    basis = jnp.broadcast_to(
        jnp.eye(head_size, dtype=jnp.float32), (heads_here, head_size, head_size)
    )
    empty_rows = jnp.zeros((heads_here, head_size, head_size), jnp.float32)
    start_rows = jnp.concatenate([empty_rows, basis], axis=1)
    end_rows, outputs = lax.scan(
        block_step,
        start_rows,
        (
            to_blocks(log_decay),
            to_blocks(-unit_keys),
            to_blocks(unit_keys * learn_rate),
            to_blocks(keys_float * learn_rate),
            to_blocks(recv_float),
            to_blocks(val_rows),
        ),
    )
    offset_part = end_rows[:, :head_size, :]
    transit = end_rows[:, head_size:, :]
    prefix = carried_in((transit, offset_part), "sp", compose, (basis, empty_rows))
    entering = prefix[1]
    direct = outputs[..., :head_size]
    through = outputs[..., head_size:]
    state_read = direct + jnp.einsum("hji,nhti->nhtj", entering, through, precision=HIGHEST)
    state_read = state_read.transpose(0, 2, 1, 3).reshape(shaped)
    centre = jnp.mean(state_read, axis=-1, keepdims=True)
    centred = state_read - centre
    variance = jnp.mean(centred * centred, axis=-1, keepdims=True)
    state_out = (
        (centred * lax.rsqrt(variance + GROUP_EPS)).reshape(tok_count, heads_here * head_size)
        * head_gain
    ).astype(jnp.bfloat16)
    local_oc, local_os = (
        lax.all_gather(out_conv, "fs", axis=1, tiled=True),
        lax.all_gather(out_state, "fs", axis=1, tiled=True),
    )
    conv_cols, state_cols = (
        lax.all_gather(local_oc, "sp", axis=1, tiled=True),
        lax.all_gather(local_os, "sp", axis=1, tiled=True),
    )
    tp_count = lax.axis_size("tp")
    own_rows = tok_count // tp_count
    merged = lax.psum_scatter(
        (
            jnp.dot(conv_out, conv_cols, preferred_element_type=jnp.float32)
            + jnp.dot(state_out, state_cols, preferred_element_type=jnp.float32)
        ).astype(jnp.bfloat16),
        "tp",
        scatter_dimension=0,
        tiled=True,
    ).astype(jnp.float32)
    return merged.astype(jnp.bfloat16).reshape(1, own_rows, merged.shape[1])

def mm(x, y, dims=(1, 0)):
    xh = x.astype(jnp.bfloat16)
    xl = (x - xh.astype(jnp.float32)).astype(jnp.bfloat16)
    yh = y.astype(jnp.bfloat16)
    yl = (y - yh.astype(jnp.float32)).astype(jnp.bfloat16)
    how = (((dims[0],), (dims[1],)), ((), ()))

    def one(p, q):
        return lax.dot_general(p, q, how, preferred_element_type=jnp.float32)

    return one(xh, yh) + (one(xh, yl) + one(xl, yh))


def range_rows(length):
    t = np.arange(length)[:, None]
    u = np.arange(length)[None, :]
    rows = []
    h = 1
    while h < length:
        start = t // h * h
        odd = (t // h) % 2 == 1
        rows.append(np.where(odd, (u >= start) & (u < t), (u > t) & (u < start + h)))
        rows.append(np.where(odd, (u >= start) & (u <= t), False))
        h *= 2
    rows.append(u < t)
    rows.append(u <= t)
    rows.append(u > t)
    rows.append(np.ones((length, length), bool))
    stacked = np.concatenate(rows, axis=0).astype(np.float32)
    return np.concatenate([stacked] * 3, axis=1)


def recur_kernel(
    length, group, ld_ref, a_ref, b_ref, k_ref, r_ref, v_ref, sel_ref, gain_ref, out_ref,
    t_buf, g_buf, q_buf, o_buf
):
    L = length
    size = ld_ref.shape[1]
    blocks = ld_ref.shape[0] // L
    levels = L.bit_length() - 1
    it = lax.broadcasted_iota(jnp.int32, (L, L), 0)
    iu = lax.broadcasted_iota(jnp.int32, (L, L), 1)

    def pair_mask(lv):
        bt = lax.shift_right_logical(it, lv)
        bu = lax.shift_right_logical(iu, lv)
        return ((bt & 1) == 1) & (bu == bt - 1)

    eye = jnp.where(it == iu, 1.0, 0.0).astype(jnp.float32)
    ek_t = lax.broadcasted_iota(jnp.int32, (size, size), 0)
    ek_u = lax.broadcasted_iota(jnp.int32, (size, size), 1)

    def chunk_group(i, _):
        base = [(i * group + g) for g in range(group)]
        at = [pl.ds(pl.multiple_of(n * L, L), L) for n in base]
        ld = [ld_ref[s, :] for s in at]
        a = [a_ref[s, :] for s in at]
        b = [b_ref[s, :] for s in at]
        k = [k_ref[s, :] for s in at]
        r = [r_ref[s, :] for s in at]
        v = [v_ref[s, :] for s in at]
        ex = []
        for x in ld:
            hi = x.astype(jnp.bfloat16)
            rest = x - hi.astype(jnp.float32)
            mid = rest.astype(jnp.bfloat16)
            low = (rest - mid.astype(jnp.float32)).astype(jnp.bfloat16)
            three = jnp.concatenate([hi, mid, low], axis=0)
            ex.append(jnp.exp(jnp.dot(sel_ref[...], three, preferred_element_type=jnp.float32)))
        acc_b = [None] * group
        acc_k = [None] * group
        for lv in range(levels + 1):
            if lv < levels:
                one = pair_mask(lv)
                mask = jnp.concatenate([one, one], axis=0)
            else:
                mask = jnp.concatenate([jnp.zeros((L, L), jnp.float32), eye], axis=0) > 0.5
            for g in range(group):
                if lv < levels:
                    e0 = ex[g][2 * lv * L : (2 * lv + 1) * L]
                    e1 = ex[g][(2 * lv + 1) * L : (2 * lv + 2) * L]
                    left = jnp.concatenate([a[g] * e0, r[g] * e1], axis=0)
                    qb, qk = b[g] * e0, k[g] * e0
                else:
                    left = jnp.concatenate([a[g], r[g]], axis=0)
                    qb, qk = b[g], k[g]
                sb = jnp.where(mask, mm(left, qb, (1, 1)), 0.0)
                sk = jnp.where(mask, mm(left, qk, (1, 1)), 0.0)
                acc_b[g] = sb if lv == 0 else acc_b[g] + sb
                acc_k[g] = sk if lv == 0 else acc_k[g] + sk
        inv = [eye + jnp.where(pair_mask(0), acc_b[g][:L], 0.0) for g in range(group)]
        for lv in range(1, levels):
            mask = pair_mask(lv)
            mid = [mm(inv[g], jnp.where(mask, acc_b[g][:L], 0.0)) for g in range(group)]
            inv = [inv[g] + mm(mid[g], inv[g]) for g in range(group)]
        tail = 2 * levels * L
        for g in range(group):
            e_ex = ex[g][tail : tail + L]
            e_in = ex[g][tail + L : tail + 2 * L]
            e_end = ex[g][tail + 2 * L : tail + 3 * L]
            e_all = ex[g][tail + 3 * L : tail + 3 * L + size]
            w = mm(inv[g], a[g] * e_ex)
            u = mm(inv[g], mm(acc_k[g][:L], v[g]))
            b_end = b[g] * e_end
            n = base[g]
            t_buf[n] = jnp.where(ek_t == ek_u, e_all, 0.0) + mm(b_end, w, (0, 0))
            g_buf[n] = mm(b_end, u, (0, 0)) + mm(k[g] * e_end, v[g], (0, 0))
            q_buf[n] = r[g] * e_in + mm(acc_b[g][L:], w)
            o_buf[n] = mm(acc_b[g][L:], u) + mm(acc_k[g][L:], v[g])
        return 0

    lax.fori_loop(0, blocks // group, chunk_group, 0)

    def pass_on(n, state):
        read = mm(q_buf[n], state) + o_buf[n]
        centred = read - jnp.mean(read, axis=-1, keepdims=True)
        variance = jnp.mean(centred * centred, axis=-1, keepdims=True)
        done = centred * lax.rsqrt(variance + GROUP_EPS) * gain_ref[...]
        out_ref[pl.ds(pl.multiple_of(n * L, L), L), :] = done.astype(out_ref.dtype)
        return mm(t_buf[n], state) + g_buf[n]

    lax.fori_loop(0, blocks, pass_on, jnp.zeros((size, size), jnp.float32))


def recurrence(log_decay, remove, write, key_rate, recv, vals, gain):
    count, size = log_decay.shape
    length = 64
    blocks = count // length
    group = 2 if blocks % 2 == 0 else 1
    sel = jnp.asarray(range_rows(length), jnp.bfloat16)
    vm = pl.BlockSpec(memory_space=pltpu.VMEM)
    return pl.pallas_call(
        partial(recur_kernel, length, group),
        out_shape=jax.ShapeDtypeStruct((count, size), jnp.bfloat16),
        in_specs=[vm] * 8,
        out_specs=vm,
        scratch_shapes=[
            pltpu.VMEM((blocks, size, size), jnp.float32),
            pltpu.VMEM((blocks, size, size), jnp.float32),
            pltpu.VMEM((blocks, length, size), jnp.float32),
            pltpu.VMEM((blocks, length, size), jnp.float32),
        ],
    )(log_decay, remove, write, key_rate, recv, vals, sel, gain.reshape(1, size))


def peers():
    sp, fs, tp = (lax.axis_size(name) for name in ("sp", "fs", "tp"))
    z, f, c = (lax.axis_index(name) for name in ("sp", "fs", "tp"))
    return sp, fs, tp, z, f, c


def greet(devices):
    barrier = pltpu.get_barrier_semaphore()
    for device in devices:
        pl.semaphore_signal(barrier, inc=1, device_id=device, device_id_type=MESH)
    pl.semaphore_wait(barrier, len(devices))


def send(src, dst, sends, recvs, device):
    copy = pltpu.make_async_remote_copy(
        src_ref=src, dst_ref=dst, send_sem=sends, recv_sem=recvs,
        device_id=device, device_id_type=MESH,
    )
    copy.start()
    return copy


def gather_kernel(
    tok_ref, w_ref, o_ref, shift_ref, toks, weights, outs, shifts,
    loc_sem, zs, zr, fs_s, fs_r, ts, tr, ps, pr, hs, hr, ozs, ozr, ofs, ofr, ops, opr
):
    sp, fs, tp, z, f, c = peers()
    across = [lax.rem(z + d, sp) for d in range(sp)]
    behind = [lax.rem(z + sp - d, sp) for d in range(sp)]
    beside = [lax.rem(f + d, fs) for d in range(fs)]
    other = 1 - c
    zdev = [(across[d], f, c) for d in range(sp)]
    fdev = [(z, beside[d], c) for d in range(fs)]
    partner = (z, f, other)
    rows, feats = tok_ref.shape
    orows, ocols = o_ref.shape
    greet(zdev[1:] + fdev[1:] + [partner])

    def tok_at(zi, ci):
        return toks.at[pl.ds(pl.multiple_of(zi * rows, rows), rows),
                       pl.ds(pl.multiple_of(ci * feats, feats), feats)]

    def out_at(zi, fi, ci):
        return outs.at[pl.ds(pl.multiple_of(ci * orows, orows), orows),
                       pl.ds(pl.multiple_of((zi * fs + fi) * ocols, ocols), ocols)]

    local = [
        pltpu.make_async_copy(w_ref.at[z], weights.at[z, f], loc_sem.at[0]),
        pltpu.make_async_copy(tok_ref, tok_at(z, c), loc_sem.at[1]),
        pltpu.make_async_copy(shift_ref.at[z], shifts.at[z], loc_sem.at[2]),
        pltpu.make_async_copy(o_ref, out_at(z, f, c), loc_sem.at[3]),
    ]
    for copy in local:
        copy.start()
    w_z = [send(w_ref.at[across[d]], weights.at[z, f], zs.at[d], zr.at[d], zdev[d])
           for d in range(1, sp)]
    s_z = [send(shift_ref.at[across[d]], shifts.at[z], hs.at[d], hr.at[d], zdev[d])
           for d in range(1, sp)]
    w_f = [send(w_ref.at[z], weights.at[z, f], fs_s.at[0, e], fs_r.at[0, e], fdev[e])
           for e in range(1, fs)]
    t_p = [send(tok_ref, tok_at(z, c), ps.at[0], pr.at[0], partner)]
    t_z = [send(tok_ref, tok_at(z, c), ts.at[d], tr.at[d], zdev[d]) for d in range(1, sp)]
    o_z = [send(o_ref, out_at(z, f, c), ozs.at[d], ozr.at[d], zdev[d]) for d in range(1, sp)]
    for d in range(1, sp):
        w_z[d - 1].wait_recv()
        got = weights.at[behind[d], f]
        w_f += [send(got, got, fs_s.at[d, e], fs_r.at[d, e], fdev[e]) for e in range(1, fs)]
    o_f = [send(o_ref, out_at(z, f, c), ofs.at[0, e], ofr.at[0, e], fdev[e])
           for e in range(1, fs)]
    o_p = [send(o_ref, out_at(z, f, c), ops.at[0, 0], opr.at[0, 0], partner)]
    for d in range(1, sp):
        t_z[d - 1].wait_recv()
        got = tok_at(behind[d], c)
        t_p.append(send(got, got, ps.at[d], pr.at[d], partner))
    for d in range(1, sp):
        o_z[d - 1].wait_recv()
        got = out_at(behind[d], f, c)
        o_f += [send(got, got, ofs.at[d, e], ofr.at[d, e], fdev[e]) for e in range(1, fs)]
        o_p.append(send(got, got, ops.at[d, 0], opr.at[d, 0], partner))
    for d in range(sp):
        for e in range(1, fs):
            o_f[d * (fs - 1) + e - 1].wait_recv()
            got = out_at(behind[d], lax.rem(f + fs - e, fs), c)
            o_p.append(send(got, got, ops.at[d, e], opr.at[d, e], partner))
    for copy in local:
        copy.wait()
    for copy in w_z + t_z + o_z + o_f:
        copy.wait_send()
    for copy in s_z + w_f + t_p + o_p:
        copy.wait()


def gather_all(tok, w, o, shift):
    sp, fs, tp = (lax.axis_size(name) for name in ("sp", "fs", "tp"))
    vm = pl.BlockSpec(memory_space=pltpu.VMEM)
    dma = pltpu.SemaphoreType.DMA
    rows, feats = tok.shape
    return pl.pallas_call(
        gather_kernel,
        out_shape=(
            jax.ShapeDtypeStruct((sp * rows, tp * feats), tok.dtype),
            jax.ShapeDtypeStruct((sp, fs) + w.shape[1:], w.dtype),
            jax.ShapeDtypeStruct((tp * o.shape[0], sp * fs * o.shape[1]), o.dtype),
            jax.ShapeDtypeStruct(shift.shape, shift.dtype),
        ),
        in_specs=[vm] * 4,
        out_specs=(vm,) * 4,
        scratch_shapes=[
            dma((4,)), dma((sp,)), dma((sp,)), dma((sp, fs)), dma((sp, fs)), dma((sp,)), dma((sp,)),
            dma((sp,)), dma((sp,)), dma((sp,)), dma((sp,)), dma((sp,)), dma((sp,)),
            dma((sp, fs)), dma((sp, fs)), dma((sp, fs)), dma((sp, fs)),
        ],
        compiler_params=pltpu.CompilerParams(collective_id=0, has_side_effects=True),
    )(tok, w, o, shift)


def swap_kernel(act_ref, got_ref, loc_sem, sends, recvs):
    sp, fs, tp, z, f, c = peers()
    rows = act_ref.shape[0] // (sp * tp)
    cols = act_ref.shape[1]
    steps = [(d, e) for d in range(sp) for e in range(tp)]
    dest = [(lax.rem(z + d, sp), lax.rem(c + e, tp)) for d, e in steps]
    greet([(dz, f, dc) for dz, dc in dest[1:]])

    def piece(dz, dc):
        return act_ref.at[pl.ds(pl.multiple_of((dz * tp + dc) * rows, rows), rows)]

    mine = got_ref.at[:, pl.ds(pl.multiple_of((c * sp + z) * cols, cols), cols)]
    own = pltpu.make_async_copy(piece(z, c), mine, loc_sem)
    own.start()
    copies = [send(piece(dz, dc), mine, sends.at[i], recvs.at[i], (dz, f, dc))
              for i, (dz, dc) in enumerate(dest) if i]
    own.wait()
    for copy in copies:
        copy.wait()


def swap_all(act):
    sp, tp = (lax.axis_size(name) for name in ("sp", "tp"))
    vm = pl.BlockSpec(memory_space=pltpu.VMEM)
    return pl.pallas_call(
        swap_kernel,
        out_shape=jax.ShapeDtypeStruct(
            (act.shape[0] // (sp * tp), act.shape[1] * sp * tp), act.dtype
        ),
        in_specs=[vm],
        out_specs=vm,
        scratch_shapes=[
            pltpu.SemaphoreType.DMA,
            pltpu.SemaphoreType.DMA((sp * tp,)),
            pltpu.SemaphoreType.DMA((sp * tp,)),
        ],
        compiler_params=pltpu.CompilerParams(collective_id=1, has_side_effects=True),
    )(act)


def head_body(
    tokens, norm_gain, conv_gate_out, conv_gate_in, conv_value, conv_taps, recv_weight,
    key_weight, value_weight, decay_base, decay_down, decay_up, decay_shift, rate_base,
    rate_down, rate_up, head_gain, out_conv, out_state,
):
    sp = lax.axis_size("sp")
    z = lax.axis_index("sp")
    tok_count = tokens.shape[1]
    size = recv_weight.shape[1] // sp
    own_rows = conv_gate_out.shape[0]
    tok = tokens.reshape(tok_count, tokens.shape[2])
    six = (conv_gate_out, conv_gate_in, conv_value, recv_weight, key_weight, value_weight)
    split = jnp.stack([m.reshape(own_rows, sp, size) for m in six], axis=2)
    w = split.transpose(1, 0, 2, 3).reshape(sp, own_rows, 6 * size)
    o_cols = out_conv.shape[1]
    o = jnp.stack(
        [out_conv.reshape(sp, size, o_cols), out_state.reshape(sp, size, o_cols)], axis=1
    ).reshape(2 * sp * size, o_cols)
    shift = decay_shift.reshape(tok_count, sp).T.reshape(sp, 1, tok_count)
    toks, weights, outs, shifts = gather_all(tok, w, o, shift)
    features = toks.astype(jnp.float32)
    normed = (
        features
        * lax.rsqrt(jnp.mean(features * features, axis=-1, keepdims=True) + RMS_EPS)
        * norm_gain
    ).astype(jnp.bfloat16)
    all_w = weights.reshape(toks.shape[1], 6 * size)
    low_w = jnp.concatenate([decay_down, rate_down], axis=1)
    proj = jnp.dot(normed, all_w, preferred_element_type=jnp.float32).astype(jnp.bfloat16)
    lows = jnp.dot(normed, low_w, preferred_element_type=jnp.float32)
    gate_out, gate_in, conv_in, recv, keys, vals = (
        proj[:, i * size : (i + 1) * size].astype(jnp.float32) for i in range(6)
    )
    inner = decay_down.shape[1]
    decay_low = jnp.tanh(lows[:, :inner]).astype(jnp.bfloat16)
    rate_low = lows[:, inner:].astype(jnp.bfloat16)

    def mine(array):
        return lax.dynamic_slice_in_dim(array, z * size, size, axis=array.ndim - 1)

    decay_pre = mine(decay_base) + jnp.dot(
        decay_low, mine(decay_up), preferred_element_type=jnp.float32
    )
    log_base = -jax.nn.softplus(-decay_pre) - 0.5
    log_decay = -jnp.exp(log_base + shifts.reshape(sp * tok_count, 1))
    rate = jax.nn.sigmoid(
        mine(rate_base) + jnp.dot(rate_low, mine(rate_up), preferred_element_type=jnp.float32)
    )
    unit = keys * lax.rsqrt(jnp.sum(keys * keys, axis=-1, keepdims=True) + UNIT_EPS)
    state_out = recurrence(
        log_decay, -unit, unit * rate, keys * rate, recv, vals, mine(head_gain)
    )
    mixed_in = gate_in * conv_in
    total = mixed_in.shape[0]
    padded = jnp.pad(mixed_in, ((2, 0), (0, 0)))
    taps = mine(conv_taps)
    convolved = (
        padded[:total] * taps[0] + padded[1 : total + 1] * taps[1] + padded[2:] * taps[2]
    )
    conv_out = (gate_out * convolved).astype(jnp.bfloat16)
    act = swap_all(jnp.concatenate([conv_out, state_out], axis=1))
    mixed = jnp.dot(act, outs, preferred_element_type=jnp.float32).astype(jnp.bfloat16)
    return mixed.reshape((1,) + mixed.shape)


def one_head_each(mesh, tokens, shift, weight):
    sp, tp = mesh.shape["sp"], mesh.shape["tp"]
    heads = shift.shape[2]
    count = tokens.shape[1] // sp
    size = weight.shape[1] // heads
    return (
        tp == 2
        and heads == sp * tp
        and tokens.shape[0] == mesh.shape["fs"]
        and size == 64
        and count % 128 == 0
        and weight.shape[0] % (sp * mesh.shape["fs"] * 16) == 0
    )


def solution(mesh):
    placed = (
        P("fs", "sp", "tp"),
        P(),
        P(("sp", "fs"), "tp"),
        P(("sp", "fs"), "tp"),
        P(("sp", "fs"), "tp"),
        P(None, "tp"),
        P(("sp", "fs"), "tp"),
        P(("sp", "fs"), "tp"),
        P(("sp", "fs"), "tp"),
        P("tp"),
        P(),
        P(None, "tp"),
        P("fs", "sp", "tp"),
        P("tp"),
        P(),
        P(None, "tp"),
        P("tp"),
        P("tp", ("sp", "fs")),
        P("tp", ("sp", "fs")),
    )
    def run(*args):
        chosen = head_body if one_head_each(mesh, args[0], args[12], args[6]) else body
        return jax.shard_map(
            chosen, mesh=mesh, in_specs=placed, out_specs=P("fs", ("sp", "tp"), None),
            check_vma=False,
        )(*args)

    return run
```

```python
from functools import partial
import math

import jax
import jax.numpy as jnp
import numpy as np
from jax import lax
from jax.experimental import pallas as pl
from jax.experimental.pallas import tpu as pltpu
from jax.sharding import PartitionSpec as P

RMS_EPS = 1e-05
GROUP_EPS = 0.00064
UNIT_EPS = 1e-06
HIGHEST = lax.Precision.HIGHEST
MESH = pl.DeviceIdType.MESH


def from_behind(array, axis, by):
    size = lax.axis_size(axis)
    pairs = [(i, i + by) for i in range(size) if 0 <= i + by < size]
    return lax.ppermute(array, axis, pairs)


def carried_in(array, axis, combine, identity):
    size, index = (lax.axis_size(axis), lax.axis_index(axis))
    everything = jax.tree.map(
        lambda part, kind: lax.all_gather(part.astype(kind), axis),
        array,
        (jnp.bfloat16, jnp.bfloat16),
    )
    start = jax.tree.map(
        lambda part, zero: jnp.broadcast_to(jnp.asarray(zero, part.dtype), part.shape),
        array,
        identity,
    )

    def lap(k, before):
        reached = k < index
        new = combine(
            before, jax.tree.map(lambda part, own: part[k].astype(own.dtype), everything, array)
        )
        return jax.tree.map(lambda a, b: jnp.where(reached, a, b), new, before)

    return lax.fori_loop(0, size, lap, start)


def fold_rows(normed, totals, pieces, offset):
    return tuple(
        (
            jnp.dot(normed, pieces[member], preferred_element_type=jnp.float32)
            for member in range(len(pieces))
        )
    )


def block_step(carried, inputs):
    log_dec, remove_dir, write_dir, key_rate, receive, val_rows = inputs
    cumulative = jnp.cumsum(log_dec, axis=1)
    exclusive = cumulative - log_dec
    length = log_dec.shape[1]
    where_t = lax.broadcasted_iota(jnp.int32, (length, length), 0)
    where_s = lax.broadcasted_iota(jnp.int32, (length, length), 1)
    strict = (where_t > where_s)[None, :, :, None]
    inclusive = (where_t >= where_s)[None, :, :, None]
    damp_prior = jnp.where(
        strict, jnp.exp(jnp.minimum(exclusive[:, :, None, :] - cumulative[:, None, :, :], 0.0)), 0.0
    )
    damp_now = jnp.where(
        inclusive,
        jnp.exp(jnp.minimum(cumulative[:, :, None, :] - cumulative[:, None, :, :], 0.0)),
        0.0,
    )
    link_ab = jnp.einsum("htc,htsc,hsc->hts", remove_dir, damp_prior, write_dir, precision=HIGHEST)
    link_ak = jnp.einsum("htc,htsc,hsc->hts", remove_dir, damp_prior, key_rate, precision=HIGHEST)
    from_start = jnp.einsum(
        "hrc,htc->htr", carried, remove_dir * jnp.exp(exclusive), precision=HIGHEST
    )
    rhs_terms = from_start + jnp.einsum("hts,hsr->htr", link_ak, val_rows, precision=HIGHEST)
    unit_matrix = jnp.eye(length, dtype=jnp.float32)
    projected = lax.linalg.triangular_solve(
        unit_matrix - link_ab, rhs_terms, left_side=True, lower=True, unit_diagonal=True
    )
    read_b = jnp.einsum("htc,htsc,hsc->hts", receive, damp_now, write_dir, precision=HIGHEST)
    read_k = jnp.einsum("htc,htsc,hsc->hts", receive, damp_now, key_rate, precision=HIGHEST)
    outputs = (
        jnp.einsum("hrc,htc->htr", carried, receive * jnp.exp(cumulative), precision=HIGHEST)
        + jnp.einsum("hts,hsr->htr", read_b, projected, precision=HIGHEST)
        + jnp.einsum("hts,hsr->htr", read_k, val_rows, precision=HIGHEST)
    )
    to_end = jnp.exp(cumulative[:, -1:, :] - cumulative)
    new_state = (
        carried * jnp.exp(cumulative[:, -1, :])[:, None, :]
        + jnp.einsum("hsr,hsc->hrc", projected, write_dir * to_end, precision=HIGHEST)
        + jnp.einsum("hsr,hsc->hrc", val_rows, key_rate * to_end, precision=HIGHEST)
    )
    return (new_state, outputs)


def compose(earlier, later):
    return (
        jnp.einsum("hij,hjk->hik", earlier[0], later[0], precision=HIGHEST),
        jnp.einsum("hij,hjk->hik", earlier[1], later[0], precision=HIGHEST) + later[1],
    )


def body(
    tokens,
    norm_gain,
    conv_gate_out,
    conv_gate_in,
    conv_value,
    conv_taps,
    recv_weight,
    key_weight,
    value_weight,
    decay_base,
    decay_down,
    decay_up,
    decay_shift,
    rate_base,
    rate_down,
    rate_up,
    head_gain,
    out_conv,
    out_state,
):
    tok_count = tokens.shape[1]
    own_half = tokens.reshape(tok_count, tokens.shape[2])
    features = lax.all_gather(own_half, "tp", axis=1, tiled=True).astype(jnp.float32)
    normed = (
        features
        * lax.rsqrt(jnp.mean(features * features, axis=-1, keepdims=True) + RMS_EPS)
        * norm_gain
    ).astype(jnp.bfloat16)
    widths = (
        conv_gate_out.shape[1],
        conv_gate_in.shape[1],
        conv_value.shape[1],
        recv_weight.shape[1],
        key_weight.shape[1],
        value_weight.shape[1],
    )
    zeros_init = tuple(
        (jnp.zeros((tok_count, column_count), jnp.float32) for column_count in widths)
    )
    row_adder = partial(fold_rows, normed)
    local_go, local_gi, local_cv, local_rw, local_kw, local_vw = (
        lax.all_gather(conv_gate_out, "fs", axis=0, tiled=True),
        lax.all_gather(conv_gate_in, "fs", axis=0, tiled=True),
        lax.all_gather(conv_value, "fs", axis=0, tiled=True),
        lax.all_gather(recv_weight, "fs", axis=0, tiled=True),
        lax.all_gather(key_weight, "fs", axis=0, tiled=True),
        lax.all_gather(value_weight, "fs", axis=0, tiled=True),
    )
    projected_sums = row_adder(
        zeros_init,
        (
            lax.all_gather(local_go, "sp", axis=0, tiled=True),
            lax.all_gather(local_gi, "sp", axis=0, tiled=True),
            lax.all_gather(local_cv, "sp", axis=0, tiled=True),
            lax.all_gather(local_rw, "sp", axis=0, tiled=True),
            lax.all_gather(local_kw, "sp", axis=0, tiled=True),
            lax.all_gather(local_vw, "sp", axis=0, tiled=True),
        ),
        jnp.int32(0),
    )
    gate_out, gate_in, conv_in, recv_raw, keys_raw, vals_raw = tuple(
        (member.astype(jnp.bfloat16) for member in projected_sums)
    )
    mixed_in = gate_in.astype(jnp.float32) * conv_in.astype(jnp.float32)
    edge_rows = from_behind(mixed_in[-2:], "sp", 1)
    padded = jnp.concatenate([edge_rows, mixed_in], axis=0)
    convolved = (
        padded[0:tok_count] * conv_taps[0]
        + padded[1 : tok_count + 1] * conv_taps[1]
        + padded[2:] * conv_taps[2]
    )
    conv_out = (gate_out.astype(jnp.float32) * convolved).astype(jnp.bfloat16)
    heads_here = decay_shift.shape[2]
    head_size = recv_raw.shape[1] // heads_here
    shaped = (tok_count, heads_here, head_size)
    decay_low = jnp.tanh(jnp.dot(normed, decay_down, preferred_element_type=jnp.float32)).astype(
        jnp.bfloat16
    )
    rate_low = jnp.dot(normed, rate_down, preferred_element_type=jnp.float32).astype(jnp.bfloat16)
    decay_pre = decay_base + jnp.dot(decay_low, decay_up, preferred_element_type=jnp.float32)
    log_base = -jax.nn.softplus(-decay_pre) - 0.5
    log_decay = -jnp.exp(log_base.reshape(shaped) + decay_shift.reshape(tok_count, heads_here, 1))
    learn_rate = jax.nn.sigmoid(
        rate_base + jnp.dot(rate_low, rate_up, preferred_element_type=jnp.float32)
    ).reshape(shaped)
    keys_float = keys_raw.astype(jnp.float32).reshape(shaped)
    unit_keys = keys_float * lax.rsqrt(
        jnp.sum(keys_float * keys_float, axis=-1, keepdims=True) + UNIT_EPS
    )
    values_float = vals_raw.astype(jnp.float32).reshape(shaped)
    recv_float = recv_raw.astype(jnp.float32).reshape(shaped)
    block_len = math.gcd(tok_count, 32)
    blocks = tok_count // block_len

    def to_blocks(field):
        return field.reshape(blocks, block_len, heads_here, field.shape[2]).transpose(0, 2, 1, 3)

    val_rows = jnp.concatenate([values_float, jnp.zeros_like(values_float)], axis=2)
    basis = jnp.broadcast_to(
        jnp.eye(head_size, dtype=jnp.float32), (heads_here, head_size, head_size)
    )
    empty_rows = jnp.zeros((heads_here, head_size, head_size), jnp.float32)
    start_rows = jnp.concatenate([empty_rows, basis], axis=1)
    end_rows, outputs = lax.scan(
        block_step,
        start_rows,
        (
            to_blocks(log_decay),
            to_blocks(-unit_keys),
            to_blocks(unit_keys * learn_rate),
            to_blocks(keys_float * learn_rate),
            to_blocks(recv_float),
            to_blocks(val_rows),
        ),
    )
    offset_part = end_rows[:, :head_size, :]
    transit = end_rows[:, head_size:, :]
    prefix = carried_in((transit, offset_part), "sp", compose, (basis, empty_rows))
    entering = prefix[1]
    direct = outputs[..., :head_size]
    through = outputs[..., head_size:]
    state_read = direct + jnp.einsum("hji,nhti->nhtj", entering, through, precision=HIGHEST)
    state_read = state_read.transpose(0, 2, 1, 3).reshape(shaped)
    centre = jnp.mean(state_read, axis=-1, keepdims=True)
    centred = state_read - centre
    variance = jnp.mean(centred * centred, axis=-1, keepdims=True)
    state_out = (
        (centred * lax.rsqrt(variance + GROUP_EPS)).reshape(tok_count, heads_here * head_size)
        * head_gain
    ).astype(jnp.bfloat16)
    local_oc, local_os = (
        lax.all_gather(out_conv, "fs", axis=1, tiled=True),
        lax.all_gather(out_state, "fs", axis=1, tiled=True),
    )
    conv_cols, state_cols = (
        lax.all_gather(local_oc, "sp", axis=1, tiled=True),
        lax.all_gather(local_os, "sp", axis=1, tiled=True),
    )
    tp_count = lax.axis_size("tp")
    own_rows = tok_count // tp_count
    merged = lax.psum_scatter(
        (
            jnp.dot(conv_out, conv_cols, preferred_element_type=jnp.float32)
            + jnp.dot(state_out, state_cols, preferred_element_type=jnp.float32)
        ).astype(jnp.bfloat16),
        "tp",
        scatter_dimension=0,
        tiled=True,
    ).astype(jnp.float32)
    return merged.astype(jnp.bfloat16).reshape(1, own_rows, merged.shape[1])

def mm(x, y, dims=(1, 0)):
    xh = x.astype(jnp.bfloat16)
    xl = (x - xh.astype(jnp.float32)).astype(jnp.bfloat16)
    yh = y.astype(jnp.bfloat16)
    yl = (y - yh.astype(jnp.float32)).astype(jnp.bfloat16)
    how = (((dims[0],), (dims[1],)), ((), ()))

    def one(p, q):
        return lax.dot_general(p, q, how, preferred_element_type=jnp.float32)

    return one(xh, yh) + (one(xh, yl) + one(xl, yh))


def range_rows(length):
    t = np.arange(length)[:, None]
    u = np.arange(length)[None, :]
    rows = []
    h = 1
    while h < length:
        start = t // h * h
        odd = (t // h) % 2 == 1
        rows.append(np.where(odd, (u >= start) & (u < t), (u > t) & (u < start + h)))
        rows.append(np.where(odd, (u >= start) & (u <= t), False))
        h *= 2
    rows.append(u < t)
    rows.append(u <= t)
    rows.append(u > t)
    rows.append(np.ones((length, length), bool))
    stacked = np.concatenate(rows, axis=0).astype(np.float32)
    return np.concatenate([stacked] * 3, axis=1)


def peers():
    sp, fs, tp = (lax.axis_size(name) for name in ("sp", "fs", "tp"))
    z, f, c = (lax.axis_index(name) for name in ("sp", "fs", "tp"))
    return sp, fs, tp, z, f, c


def greet(devices):
    barrier = pltpu.get_barrier_semaphore()
    for device in devices:
        pl.semaphore_signal(barrier, inc=1, device_id=device, device_id_type=MESH)
    pl.semaphore_wait(barrier, len(devices))


def send(src, dst, sends, recvs, device):
    copy = pltpu.make_async_remote_copy(
        src_ref=src, dst_ref=dst, send_sem=sends, recv_sem=recvs,
        device_id=device, device_id_type=MESH,
    )
    copy.start()
    return copy


def pair_mask(length, lv):
    bt = lax.shift_right_logical(lax.broadcasted_iota(jnp.int32, (length, length), 0), lv)
    bu = lax.shift_right_logical(lax.broadcasted_iota(jnp.int32, (length, length), 1), lv)
    return ((bt & 1) == 1) & (bu == bt - 1)


def unit_matrix(size):
    it = lax.broadcasted_iota(jnp.int32, (size, size), 0)
    iu = lax.broadcasted_iota(jnp.int32, (size, size), 1)
    return jnp.where(it == iu, 1.0, 0.0).astype(jnp.float32)


def blocks_of(first, group, L, fields, sel_ref, bufs):
    t_buf, g_buf, q_buf, o_buf = bufs
    levels = L.bit_length() - 1
    base = [first + g for g in range(group)]
    at = [pl.ds(pl.multiple_of(n * L, L), L) for n in base]
    ld, a, b, k, r, v = ([ref[s, :] for s in at] for ref in fields)
    size = ld[0].shape[1]
    eye = unit_matrix(L)
    ex = []
    for x in ld:
        hi = x.astype(jnp.bfloat16)
        rest = x - hi.astype(jnp.float32)
        mid = rest.astype(jnp.bfloat16)
        low = (rest - mid.astype(jnp.float32)).astype(jnp.bfloat16)
        three = jnp.concatenate([hi, mid, low], axis=0)
        ex.append(jnp.exp(jnp.dot(sel_ref[...], three, preferred_element_type=jnp.float32)))
    acc_b = [None] * group
    acc_k = [None] * group
    for lv in range(levels + 1):
        if lv < levels:
            one = pair_mask(L, lv)
            mask = jnp.concatenate([one, one], axis=0)
        else:
            mask = jnp.concatenate([jnp.zeros((L, L), jnp.float32), eye], axis=0) > 0.5
        for g in range(group):
            if lv < levels:
                e0 = ex[g][2 * lv * L : (2 * lv + 1) * L]
                e1 = ex[g][(2 * lv + 1) * L : (2 * lv + 2) * L]
                left = jnp.concatenate([a[g] * e0, r[g] * e1], axis=0)
                qb, qk = b[g] * e0, k[g] * e0
            else:
                left = jnp.concatenate([a[g], r[g]], axis=0)
                qb, qk = b[g], k[g]
            sb = jnp.where(mask, mm(left, qb, (1, 1)), 0.0)
            sk = jnp.where(mask, mm(left, qk, (1, 1)), 0.0)
            acc_b[g] = sb if lv == 0 else acc_b[g] + sb
            acc_k[g] = sk if lv == 0 else acc_k[g] + sk
    inv = [eye + jnp.where(pair_mask(L, 0), acc_b[g][:L], 0.0) for g in range(group)]
    for lv in range(1, levels):
        mask = pair_mask(L, lv)
        half = [mm(inv[g], jnp.where(mask, acc_b[g][:L], 0.0)) for g in range(group)]
        inv = [inv[g] + mm(half[g], inv[g]) for g in range(group)]
    tail = 2 * levels * L
    for g in range(group):
        e_ex = ex[g][tail : tail + L]
        e_in = ex[g][tail + L : tail + 2 * L]
        e_end = ex[g][tail + 2 * L : tail + 3 * L]
        e_all = ex[g][tail + 3 * L : tail + 3 * L + size]
        w = mm(inv[g], a[g] * e_ex)
        u = mm(inv[g], mm(acc_k[g][:L], v[g]))
        b_end = b[g] * e_end
        n = base[g]
        t_buf[n] = unit_matrix(size) * e_all + mm(b_end, w, (0, 0))
        g_buf[n] = mm(b_end, u, (0, 0)) + mm(k[g] * e_end, v[g], (0, 0))
        q_buf[n] = r[g] * e_in + mm(acc_b[g][L:], w)
        o_buf[n] = mm(acc_b[g][L:], u) + mm(acc_k[g][L:], v[g])


def sigmoid(x):
    return jnp.exp(jnp.minimum(x, 0.0)) / (1.0 + jnp.exp(-jnp.abs(x)))


def halves(tile):
    size = tile.shape[1] // 2
    return tile[:, :size], pltpu.roll(tile, size, 1)[:, :size]


def layer_kernel(
    tok_ref, go_ref, gi_ref, cv_ref, rw_ref, kw_ref, vw_ref, oc_ref, os_ref, shift_ref,
    norm_ref, low_ref, up_ref, base_ref, taps_ref, gain_ref, sel_ref, out_ref,
    toks, w_ref, weights, o_ref, outs, shifts, ld_ref, a_ref, b_ref, k_ref, r_ref, v_ref,
    gate_ref, mixed_ref, t_buf, g_buf, q_buf, o_buf, act_ref, got_ref,
    loc_sem, zs, zr, fs_s, fs_r, ts, tr, ps, pr, hs, hr, ozs, ozr, ofs, ofr, ops, opr,
    act_s, act_r,
):
    sp, fs, tp, z, f, c = peers()
    across = [lax.rem(z + d, sp) for d in range(sp)]
    behind = [lax.rem(z + sp - d, sp) for d in range(sp)]
    beside = [lax.rem(f + d, fs) for d in range(fs)]
    other = 1 - c
    zdev = [(across[d], f, c) for d in range(sp)]
    fdev = [(z, beside[d], c) for d in range(fs)]
    partner = (z, f, other)
    rows, feats = tok_ref.shape
    orows, ocols = o_ref.shape
    wide = 2 * (go_ref.shape[1] // sp)
    size = wide // 2
    L = 64
    count = sp * rows
    nblocks = count // L

    lane = lax.broadcasted_iota(jnp.int32, (go_ref.shape[0], wide), 1)
    pairs = ((go_ref, gi_ref), (cv_ref, rw_ref), (kw_ref, vw_ref))
    for p, (first, second) in enumerate(pairs):
        for t in range(sp // 2):
            x = first[:, t * wide : (t + 1) * wide].astype(jnp.float32)
            y = second[:, t * wide : (t + 1) * wide].astype(jnp.float32)
            cols = pl.ds(p * wide, wide)
            even = jnp.where(lane < size, x, pltpu.roll(y, size, 1))
            odd = jnp.where(lane < size, pltpu.roll(x, size, 1), y)
            w_ref[2 * t, :, cols] = even.astype(jnp.bfloat16)
            w_ref[2 * t + 1, :, cols] = odd.astype(jnp.bfloat16)
    for t in range(sp):
        o_ref[2 * t * size : (2 * t + 1) * size, :] = oc_ref[t * size : (t + 1) * size, :]
        o_ref[(2 * t + 1) * size : (2 * t + 2) * size, :] = os_ref[t * size : (t + 1) * size, :]
    mixed_ref[0:8, :] = jnp.zeros((8, size), jnp.float32)

    line = [(lax.rem(z + d, sp), f, lax.rem(c + e, tp)) for d in range(sp) for e in range(tp)]
    greet(line[1:] + fdev[1:])

    def tok_at(zi, ci):
        return toks.at[pl.ds(pl.multiple_of(zi * rows, rows), rows),
                       pl.ds(pl.multiple_of(ci * feats, feats), feats)]

    def out_at(zi, fi, ci):
        return outs.at[pl.ds(pl.multiple_of(ci * orows, orows), orows),
                       pl.ds(pl.multiple_of((zi * fs + fi) * ocols, ocols), ocols)]

    local = [
        pltpu.make_async_copy(w_ref.at[z], weights.at[z, f], loc_sem.at[0]),
        pltpu.make_async_copy(tok_ref, tok_at(z, c), loc_sem.at[1]),
        pltpu.make_async_copy(shift_ref.at[z], shifts.at[z], loc_sem.at[2]),
        pltpu.make_async_copy(o_ref, out_at(z, f, c), loc_sem.at[3]),
    ]
    w_z = [send(w_ref.at[across[d]], weights.at[z, f], zs.at[d], zr.at[d], zdev[d])
           for d in range(1, sp)]
    s_z = [send(shift_ref.at[across[d]], shifts.at[z], hs.at[d], hr.at[d], zdev[d])
           for d in range(1, sp)]
    w_f = [[send(w_ref.at[z], weights.at[z, f], fs_s.at[0, e], fs_r.at[0, e], fdev[e])
            for e in range(1, fs)]]
    t_p = [send(tok_ref, tok_at(z, c), ps.at[0], pr.at[0], partner)]
    t_z = [send(tok_ref, tok_at(z, c), ts.at[d], tr.at[d], zdev[d]) for d in range(1, sp)]
    o_z = [send(o_ref, out_at(z, f, c), ozs.at[d], ozr.at[d], zdev[d]) for d in range(1, sp)]
    for copy in local:
        copy.start()
    for d in range(1, sp):
        w_z[d - 1].wait_recv()
        got = weights.at[behind[d], f]
        w_f.append([send(got, got, fs_s.at[d, e], fs_r.at[d, e], fdev[e]) for e in range(1, fs)])
    o_f = [send(o_ref, out_at(z, f, c), ofs.at[0, e], ofr.at[0, e], fdev[e])
           for e in range(1, fs)]
    o_p = [send(o_ref, out_at(z, f, c), ops.at[0, 0], opr.at[0, 0], partner)]
    for d in range(1, sp):
        t_z[d - 1].wait_recv()
        got = tok_at(behind[d], c)
        t_p.append(send(got, got, ps.at[d], pr.at[d], partner))
    for copy in local:
        copy.wait()
    for copies in w_f:
        for copy in copies:
            copy.wait_recv()

    def pass_out(d):
        o_z[d - 1].wait_recv()
        got = out_at(behind[d], f, c)
        o_p.append(send(got, got, ops.at[d, 0], opr.at[d, 0], partner))
        o_f.extend(send(got, got, ofs.at[d, e], ofr.at[d, e], fdev[e]) for e in range(1, fs))

    all_w = weights[...].reshape(sp * fs * w_ref.shape[1], w_ref.shape[2])
    for d in range(sp):
        t_p[d].wait_recv()
        if d:
            s_z[d - 1].wait_recv()
        start = pl.multiple_of(behind[d] * rows, rows)
        here = pl.ds(start, rows)
        x = toks[here, :].astype(jnp.float32)
        normed = (
            x * lax.rsqrt(jnp.mean(x * x, axis=-1, keepdims=True) + RMS_EPS) * norm_ref[...]
        ).astype(jnp.bfloat16)
        proj = jnp.dot(normed, all_w, preferred_element_type=jnp.float32)
        proj = proj.astype(jnp.bfloat16).astype(jnp.float32)
        lows = jnp.dot(normed, low_ref[...], preferred_element_type=jnp.float32)
        low_lane = lax.broadcasted_iota(jnp.int32, lows.shape, 1)
        lows = jnp.where(low_lane < lows.shape[1] // 2, jnp.tanh(lows), lows)
        pre = base_ref[...] + jnp.dot(
            lows.astype(jnp.bfloat16), up_ref[...], preferred_element_type=jnp.float32
        )
        decay_sig, rate = halves(sigmoid(pre))
        gate_out, gate_in = halves(proj[:, :wide])
        conv_in, recv = halves(proj[:, wide : 2 * wide])
        keys, vals = halves(proj[:, 2 * wide :])
        column = jnp.transpose(shifts[behind[d]])[:, 0:1]
        ld_ref[here, :] = -decay_sig * jnp.exp(column - 0.5)
        unit = keys * lax.rsqrt(jnp.sum(keys * keys, axis=-1, keepdims=True) + UNIT_EPS)
        a_ref[here, :] = -unit
        b_ref[here, :] = unit * rate
        k_ref[here, :] = keys * rate
        r_ref[here, :] = recv
        v_ref[here, :] = vals
        gate_ref[here, :] = gate_out
        mixed_ref[pl.ds(pl.multiple_of(start + 8, 8), rows), :] = gate_in * conv_in

    fields = (ld_ref, a_ref, b_ref, k_ref, r_ref, v_ref)
    bufs = (t_buf, g_buf, q_buf, o_buf)
    group = 2
    trips = nblocks // group
    cuts = [trips * i // sp for i in range(sp + 1)]
    for i in range(sp):
        def several(n, _):
            blocks_of(n * group, group, L, fields, sel_ref, bufs)
            return 0

        lax.fori_loop(cuts[i], cuts[i + 1], several, 0)
        if i:
            pass_out(i)

    me = z * tp + c
    mine = got_ref.at[:, pl.ds(pl.multiple_of((c * sp + z) * wide, wide), wide)]

    def act_copy(n):
        return pltpu.make_async_remote_copy(
            src_ref=act_ref.at[n], dst_ref=mine, send_sem=act_s.at[n], recv_sem=act_r.at[me],
            device_id=(n // tp, f, n % tp), device_id_type=MESH,
        )

    def own_copy(n):
        return pltpu.make_async_copy(act_ref.at[n], mine, act_s.at[n])

    def give(n):
        @pl.when(me != n)
        def _():
            act_copy(n).start()

        @pl.when(me == n)
        def _():
            own_copy(n).start()

    state = jnp.zeros((size, size), jnp.float32)
    taps = taps_ref[...]
    for n in range(nblocks):
        read = mm(q_buf[n], state) + o_buf[n]
        state = mm(t_buf[n], state) + g_buf[n]
        centred = read - jnp.mean(read, axis=-1, keepdims=True)
        variance = jnp.mean(centred * centred, axis=-1, keepdims=True)
        done = centred * lax.rsqrt(variance + GROUP_EPS) * gain_ref[...]
        spot = n * L + 8
        convolved = (
            mixed_ref[spot - 2 : spot - 2 + L, :] * taps[0:1]
            + mixed_ref[spot - 1 : spot - 1 + L, :] * taps[1:2]
            + mixed_ref[spot : spot + L, :] * taps[2:3]
        )
        conv = gate_ref[n * L : (n + 1) * L, :] * convolved
        act_ref[n] = jnp.concatenate([conv, done], axis=1).astype(jnp.bfloat16)
        if n:
            give(n - 1)
    for d in range(sp):
        for e in range(1, fs):
            o_f[d * (fs - 1) + e - 1].wait_recv()
            got = out_at(behind[d], lax.rem(f + fs - e, fs), c)
            o_p.append(send(got, got, ops.at[d, e], opr.at[d, e], partner))
        if d == 0:
            give(nblocks - 1)
    for n in range(nblocks):
        @pl.when(me != n)
        def _():
            act_copy(n).wait_send()
            pltpu.make_async_remote_copy(
                src_ref=act_ref.at[n],
                dst_ref=got_ref.at[:, pl.ds(((n % tp) * sp + n // tp) * wide, wide)],
                send_sem=act_s.at[n], recv_sem=act_r.at[n],
                device_id=partner, device_id_type=MESH,
            ).wait_recv()

        @pl.when(me == n)
        def _():
            own_copy(n).wait()
    for copy in o_p:
        copy.wait()
    step = 512

    def columns(i, _):
        cols = pl.ds(pl.multiple_of(i * step, step), step)
        out_ref[:, cols] = jnp.dot(
            got_ref[...], outs[:, cols], preferred_element_type=jnp.float32
        ).astype(out_ref.dtype)
        return 0

    lax.fori_loop(0, outs.shape[1] // step, columns, 0)
    for copy in w_z + t_z + o_z + o_f + s_z:
        copy.wait_send()
    for copies in w_f:
        for copy in copies:
            copy.wait_send()
    for copy in t_p:
        copy.wait_send()


def head_body(
    tokens, norm_gain, conv_gate_out, conv_gate_in, conv_value, conv_taps, recv_weight,
    key_weight, value_weight, decay_base, decay_down, decay_up, decay_shift, rate_base,
    rate_down, rate_up, head_gain, out_conv, out_state,
):
    sp, fs, tp = (lax.axis_size(name) for name in ("sp", "fs", "tp"))
    z = lax.axis_index("sp")
    rows = tokens.shape[1]
    size = recv_weight.shape[1] // sp
    own_rows = conv_gate_out.shape[0]
    tok = tokens.reshape(rows, tokens.shape[2])
    shift = jnp.pad(decay_shift.reshape(rows, sp).T.reshape(sp, 1, rows), ((0, 0), (0, 7), (0, 0)))
    low_w = jnp.concatenate([decay_down, rate_down], axis=1)

    def mine(array):
        return lax.dynamic_slice_in_dim(array, z * size, size, axis=array.ndim - 1)

    up_d, up_r = mine(decay_up), mine(rate_up)
    up = jnp.concatenate(
        [jnp.concatenate([up_d, jnp.zeros_like(up_r)], axis=1),
         jnp.concatenate([jnp.zeros_like(up_d), up_r], axis=1)], axis=0)
    base = jnp.concatenate([mine(decay_base), mine(rate_base)]).reshape(1, 2 * size)
    length = 64
    count = sp * rows
    nblocks = count // length
    sel = jnp.asarray(range_rows(length), jnp.bfloat16)
    vm = pl.BlockSpec(memory_space=pltpu.VMEM)
    dma = pltpu.SemaphoreType.DMA
    o_rows, o_cols = 2 * out_conv.shape[0], out_conv.shape[1]
    model = out_conv.shape[1] * sp * fs
    f32, bf16 = jnp.float32, jnp.bfloat16
    field = pltpu.VMEM((count, size), f32)
    block = pltpu.VMEM((nblocks, length, size), f32)
    mixed = pl.pallas_call(
        layer_kernel,
        out_shape=jax.ShapeDtypeStruct((count // (sp * tp), model), bf16),
        in_specs=[vm] * 17,
        out_specs=vm,
        scratch_shapes=[
            pltpu.VMEM((count, tp * tok.shape[1]), bf16),
            pltpu.VMEM((sp, own_rows, 6 * size), bf16),
            pltpu.VMEM((sp, fs, own_rows, 6 * size), bf16),
            pltpu.VMEM((o_rows, o_cols), bf16),
            pltpu.VMEM((tp * o_rows, model), bf16),
            pltpu.VMEM(shift.shape, f32),
            field, field, field, field, field, field, field,
            pltpu.VMEM((count + 8, size), f32),
            block, block, block, block,
            pltpu.VMEM((nblocks, length, 2 * size), bf16),
            pltpu.VMEM((length, tp * o_rows), bf16),
            dma((4,)), dma((sp,)), dma((sp,)), dma((sp, fs)), dma((sp, fs)), dma((sp,)), dma((sp,)),
            dma((sp,)), dma((sp,)), dma((sp,)), dma((sp,)), dma((sp,)), dma((sp,)),
            dma((sp, fs)), dma((sp, fs)), dma((sp, fs)), dma((sp, fs)),
            dma((nblocks,)), dma((nblocks,)),
        ],
        compiler_params=pltpu.CompilerParams(
            collective_id=0, has_side_effects=True, vmem_limit_bytes=56 * 1024 * 1024
        ),
    )(
        tok, conv_gate_out, conv_gate_in, conv_value, recv_weight, key_weight, value_weight,
        out_conv, out_state, shift, norm_gain.reshape(1, -1), low_w, up, base,
        mine(conv_taps), mine(head_gain).reshape(1, size), sel,
    )
    return mixed.reshape((1,) + mixed.shape)


def one_head_each(mesh, tokens, shift, weight):
    sp, tp = mesh.shape["sp"], mesh.shape["tp"]
    heads = shift.shape[2]
    count = tokens.shape[1] // sp
    size = weight.shape[1] // heads
    return (
        tp == 2
        and heads == sp * tp
        and tokens.shape[0] == mesh.shape["fs"]
        and size == 64
        and count == tp * 64
        and sp % 2 == 0
        and weight.shape[0] % (sp * mesh.shape["fs"] * 16) == 0
    )


def solution(mesh):
    placed = (
        P("fs", "sp", "tp"),
        P(),
        P(("sp", "fs"), "tp"),
        P(("sp", "fs"), "tp"),
        P(("sp", "fs"), "tp"),
        P(None, "tp"),
        P(("sp", "fs"), "tp"),
        P(("sp", "fs"), "tp"),
        P(("sp", "fs"), "tp"),
        P("tp"),
        P(),
        P(None, "tp"),
        P("fs", "sp", "tp"),
        P("tp"),
        P(),
        P(None, "tp"),
        P("tp"),
        P("tp", ("sp", "fs")),
        P("tp", ("sp", "fs")),
    )
    def run(*args):
        chosen = head_body if one_head_each(mesh, args[0], args[12], args[6]) else body
        return jax.shard_map(
            chosen, mesh=mesh, in_specs=placed, out_specs=P("fs", ("sp", "tp"), None),
            check_vma=False,
        )(*args)

    return run
```

```python
from functools import partial
import math

import jax
import jax.numpy as jnp
import numpy as np
from jax import lax
from jax.experimental import pallas as pl
from jax.experimental.pallas import tpu as pltpu
from jax.sharding import PartitionSpec as P

RMS_EPS = 1e-05
GROUP_EPS = 0.00064
UNIT_EPS = 1e-06
HIGHEST = lax.Precision.HIGHEST
MESH = pl.DeviceIdType.MESH


def from_behind(array, axis, by):
    size = lax.axis_size(axis)
    pairs = [(i, i + by) for i in range(size) if 0 <= i + by < size]
    return lax.ppermute(array, axis, pairs)


def carried_in(array, axis, combine, identity):
    size, index = (lax.axis_size(axis), lax.axis_index(axis))
    everything = jax.tree.map(
        lambda part, kind: lax.all_gather(part.astype(kind), axis),
        array,
        (jnp.bfloat16, jnp.bfloat16),
    )
    start = jax.tree.map(
        lambda part, zero: jnp.broadcast_to(jnp.asarray(zero, part.dtype), part.shape),
        array,
        identity,
    )

    def lap(k, before):
        reached = k < index
        new = combine(
            before, jax.tree.map(lambda part, own: part[k].astype(own.dtype), everything, array)
        )
        return jax.tree.map(lambda a, b: jnp.where(reached, a, b), new, before)

    return lax.fori_loop(0, size, lap, start)


def fold_rows(normed, totals, pieces, offset):
    return tuple(
        (
            jnp.dot(normed, pieces[member], preferred_element_type=jnp.float32)
            for member in range(len(pieces))
        )
    )


def block_step(carried, inputs):
    log_dec, remove_dir, write_dir, key_rate, receive, val_rows = inputs
    cumulative = jnp.cumsum(log_dec, axis=1)
    exclusive = cumulative - log_dec
    length = log_dec.shape[1]
    where_t = lax.broadcasted_iota(jnp.int32, (length, length), 0)
    where_s = lax.broadcasted_iota(jnp.int32, (length, length), 1)
    strict = (where_t > where_s)[None, :, :, None]
    inclusive = (where_t >= where_s)[None, :, :, None]
    damp_prior = jnp.where(
        strict, jnp.exp(jnp.minimum(exclusive[:, :, None, :] - cumulative[:, None, :, :], 0.0)), 0.0
    )
    damp_now = jnp.where(
        inclusive,
        jnp.exp(jnp.minimum(cumulative[:, :, None, :] - cumulative[:, None, :, :], 0.0)),
        0.0,
    )
    link_ab = jnp.einsum("htc,htsc,hsc->hts", remove_dir, damp_prior, write_dir, precision=HIGHEST)
    link_ak = jnp.einsum("htc,htsc,hsc->hts", remove_dir, damp_prior, key_rate, precision=HIGHEST)
    from_start = jnp.einsum(
        "hrc,htc->htr", carried, remove_dir * jnp.exp(exclusive), precision=HIGHEST
    )
    rhs_terms = from_start + jnp.einsum("hts,hsr->htr", link_ak, val_rows, precision=HIGHEST)
    unit_matrix = jnp.eye(length, dtype=jnp.float32)
    projected = lax.linalg.triangular_solve(
        unit_matrix - link_ab, rhs_terms, left_side=True, lower=True, unit_diagonal=True
    )
    read_b = jnp.einsum("htc,htsc,hsc->hts", receive, damp_now, write_dir, precision=HIGHEST)
    read_k = jnp.einsum("htc,htsc,hsc->hts", receive, damp_now, key_rate, precision=HIGHEST)
    outputs = (
        jnp.einsum("hrc,htc->htr", carried, receive * jnp.exp(cumulative), precision=HIGHEST)
        + jnp.einsum("hts,hsr->htr", read_b, projected, precision=HIGHEST)
        + jnp.einsum("hts,hsr->htr", read_k, val_rows, precision=HIGHEST)
    )
    to_end = jnp.exp(cumulative[:, -1:, :] - cumulative)
    new_state = (
        carried * jnp.exp(cumulative[:, -1, :])[:, None, :]
        + jnp.einsum("hsr,hsc->hrc", projected, write_dir * to_end, precision=HIGHEST)
        + jnp.einsum("hsr,hsc->hrc", val_rows, key_rate * to_end, precision=HIGHEST)
    )
    return (new_state, outputs)


def compose(earlier, later):
    return (
        jnp.einsum("hij,hjk->hik", earlier[0], later[0], precision=HIGHEST),
        jnp.einsum("hij,hjk->hik", earlier[1], later[0], precision=HIGHEST) + later[1],
    )


def body(
    tokens,
    norm_gain,
    conv_gate_out,
    conv_gate_in,
    conv_value,
    conv_taps,
    recv_weight,
    key_weight,
    value_weight,
    decay_base,
    decay_down,
    decay_up,
    decay_shift,
    rate_base,
    rate_down,
    rate_up,
    head_gain,
    out_conv,
    out_state,
):
    tok_count = tokens.shape[1]
    own_half = tokens.reshape(tok_count, tokens.shape[2])
    features = lax.all_gather(own_half, "tp", axis=1, tiled=True).astype(jnp.float32)
    normed = (
        features
        * lax.rsqrt(jnp.mean(features * features, axis=-1, keepdims=True) + RMS_EPS)
        * norm_gain
    ).astype(jnp.bfloat16)
    widths = (
        conv_gate_out.shape[1],
        conv_gate_in.shape[1],
        conv_value.shape[1],
        recv_weight.shape[1],
        key_weight.shape[1],
        value_weight.shape[1],
    )
    zeros_init = tuple(
        (jnp.zeros((tok_count, column_count), jnp.float32) for column_count in widths)
    )
    row_adder = partial(fold_rows, normed)
    local_go, local_gi, local_cv, local_rw, local_kw, local_vw = (
        lax.all_gather(conv_gate_out, "fs", axis=0, tiled=True),
        lax.all_gather(conv_gate_in, "fs", axis=0, tiled=True),
        lax.all_gather(conv_value, "fs", axis=0, tiled=True),
        lax.all_gather(recv_weight, "fs", axis=0, tiled=True),
        lax.all_gather(key_weight, "fs", axis=0, tiled=True),
        lax.all_gather(value_weight, "fs", axis=0, tiled=True),
    )
    projected_sums = row_adder(
        zeros_init,
        (
            lax.all_gather(local_go, "sp", axis=0, tiled=True),
            lax.all_gather(local_gi, "sp", axis=0, tiled=True),
            lax.all_gather(local_cv, "sp", axis=0, tiled=True),
            lax.all_gather(local_rw, "sp", axis=0, tiled=True),
            lax.all_gather(local_kw, "sp", axis=0, tiled=True),
            lax.all_gather(local_vw, "sp", axis=0, tiled=True),
        ),
        jnp.int32(0),
    )
    gate_out, gate_in, conv_in, recv_raw, keys_raw, vals_raw = tuple(
        (member.astype(jnp.bfloat16) for member in projected_sums)
    )
    mixed_in = gate_in.astype(jnp.float32) * conv_in.astype(jnp.float32)
    edge_rows = from_behind(mixed_in[-2:], "sp", 1)
    padded = jnp.concatenate([edge_rows, mixed_in], axis=0)
    convolved = (
        padded[0:tok_count] * conv_taps[0]
        + padded[1 : tok_count + 1] * conv_taps[1]
        + padded[2:] * conv_taps[2]
    )
    conv_out = (gate_out.astype(jnp.float32) * convolved).astype(jnp.bfloat16)
    heads_here = decay_shift.shape[2]
    head_size = recv_raw.shape[1] // heads_here
    shaped = (tok_count, heads_here, head_size)
    decay_low = jnp.tanh(jnp.dot(normed, decay_down, preferred_element_type=jnp.float32)).astype(
        jnp.bfloat16
    )
    rate_low = jnp.dot(normed, rate_down, preferred_element_type=jnp.float32).astype(jnp.bfloat16)
    decay_pre = decay_base + jnp.dot(decay_low, decay_up, preferred_element_type=jnp.float32)
    log_base = -jax.nn.softplus(-decay_pre) - 0.5
    log_decay = -jnp.exp(log_base.reshape(shaped) + decay_shift.reshape(tok_count, heads_here, 1))
    learn_rate = jax.nn.sigmoid(
        rate_base + jnp.dot(rate_low, rate_up, preferred_element_type=jnp.float32)
    ).reshape(shaped)
    keys_float = keys_raw.astype(jnp.float32).reshape(shaped)
    unit_keys = keys_float * lax.rsqrt(
        jnp.sum(keys_float * keys_float, axis=-1, keepdims=True) + UNIT_EPS
    )
    values_float = vals_raw.astype(jnp.float32).reshape(shaped)
    recv_float = recv_raw.astype(jnp.float32).reshape(shaped)
    block_len = math.gcd(tok_count, 32)
    blocks = tok_count // block_len

    def to_blocks(field):
        return field.reshape(blocks, block_len, heads_here, field.shape[2]).transpose(0, 2, 1, 3)

    val_rows = jnp.concatenate([values_float, jnp.zeros_like(values_float)], axis=2)
    basis = jnp.broadcast_to(
        jnp.eye(head_size, dtype=jnp.float32), (heads_here, head_size, head_size)
    )
    empty_rows = jnp.zeros((heads_here, head_size, head_size), jnp.float32)
    start_rows = jnp.concatenate([empty_rows, basis], axis=1)
    end_rows, outputs = lax.scan(
        block_step,
        start_rows,
        (
            to_blocks(log_decay),
            to_blocks(-unit_keys),
            to_blocks(unit_keys * learn_rate),
            to_blocks(keys_float * learn_rate),
            to_blocks(recv_float),
            to_blocks(val_rows),
        ),
    )
    offset_part = end_rows[:, :head_size, :]
    transit = end_rows[:, head_size:, :]
    prefix = carried_in((transit, offset_part), "sp", compose, (basis, empty_rows))
    entering = prefix[1]
    direct = outputs[..., :head_size]
    through = outputs[..., head_size:]
    state_read = direct + jnp.einsum("hji,nhti->nhtj", entering, through, precision=HIGHEST)
    state_read = state_read.transpose(0, 2, 1, 3).reshape(shaped)
    centre = jnp.mean(state_read, axis=-1, keepdims=True)
    centred = state_read - centre
    variance = jnp.mean(centred * centred, axis=-1, keepdims=True)
    state_out = (
        (centred * lax.rsqrt(variance + GROUP_EPS)).reshape(tok_count, heads_here * head_size)
        * head_gain
    ).astype(jnp.bfloat16)
    local_oc, local_os = (
        lax.all_gather(out_conv, "fs", axis=1, tiled=True),
        lax.all_gather(out_state, "fs", axis=1, tiled=True),
    )
    conv_cols, state_cols = (
        lax.all_gather(local_oc, "sp", axis=1, tiled=True),
        lax.all_gather(local_os, "sp", axis=1, tiled=True),
    )
    tp_count = lax.axis_size("tp")
    own_rows = tok_count // tp_count
    merged = lax.psum_scatter(
        (
            jnp.dot(conv_out, conv_cols, preferred_element_type=jnp.float32)
            + jnp.dot(state_out, state_cols, preferred_element_type=jnp.float32)
        ).astype(jnp.bfloat16),
        "tp",
        scatter_dimension=0,
        tiled=True,
    ).astype(jnp.float32)
    return merged.astype(jnp.bfloat16).reshape(1, own_rows, merged.shape[1])

def mm(x, y, dims=(1, 0)):
    xh = x.astype(jnp.bfloat16)
    xl = (x - xh.astype(jnp.float32)).astype(jnp.bfloat16)
    yh = y.astype(jnp.bfloat16)
    yl = (y - yh.astype(jnp.float32)).astype(jnp.bfloat16)
    how = (((dims[0],), (dims[1],)), ((), ()))

    def one(p, q):
        return lax.dot_general(p, q, how, preferred_element_type=jnp.float32)

    return one(xh, yh) + (one(xh, yl) + one(xl, yh))


def range_rows(length):
    t = np.arange(length)[:, None]
    u = np.arange(length)[None, :]
    rows = []
    h = 1
    while h < length:
        start = t // h * h
        odd = (t // h) % 2 == 1
        rows.append(np.where(odd, (u >= start) & (u < t), (u > t) & (u < start + h)))
        rows.append(np.where(odd, (u >= start) & (u <= t), False))
        h *= 2
    rows.append(u < t)
    rows.append(u <= t)
    rows.append(u > t)
    rows.append(np.ones((length, length), bool))
    stacked = np.concatenate(rows, axis=0).astype(np.float32)
    return np.concatenate([stacked] * 3, axis=1)


def peers():
    sp, fs, tp = (lax.axis_size(name) for name in ("sp", "fs", "tp"))
    z, f, c = (lax.axis_index(name) for name in ("sp", "fs", "tp"))
    return sp, fs, tp, z, f, c


def greet(devices):
    barrier = pltpu.get_barrier_semaphore()
    for device in devices:
        pl.semaphore_signal(barrier, inc=1, device_id=device, device_id_type=MESH)
    pl.semaphore_wait(barrier, len(devices))


def send(src, dst, sends, recvs, device):
    copy = pltpu.make_async_remote_copy(
        src_ref=src, dst_ref=dst, send_sem=sends, recv_sem=recvs,
        device_id=device, device_id_type=MESH,
    )
    copy.start()
    return copy


def pair_mask(length, lv):
    bt = lax.shift_right_logical(lax.broadcasted_iota(jnp.int32, (length, length), 0), lv)
    bu = lax.shift_right_logical(lax.broadcasted_iota(jnp.int32, (length, length), 1), lv)
    return ((bt & 1) == 1) & (bu == bt - 1)


def unit_matrix(size):
    it = lax.broadcasted_iota(jnp.int32, (size, size), 0)
    iu = lax.broadcasted_iota(jnp.int32, (size, size), 1)
    return jnp.where(it == iu, 1.0, 0.0).astype(jnp.float32)


def blocks_of(first, group, L, fields, sel_ref, bufs):
    t_buf, g_buf, q_buf, o_buf = bufs
    levels = L.bit_length() - 1
    base = [first + g for g in range(group)]
    at = [pl.ds(pl.multiple_of(n * L, L), L) for n in base]
    ld, a, b, k, r, v = ([ref[s, :] for s in at] for ref in fields)
    size = ld[0].shape[1]
    eye = unit_matrix(L)
    ex = []
    for x in ld:
        hi = x.astype(jnp.bfloat16)
        rest = x - hi.astype(jnp.float32)
        mid = rest.astype(jnp.bfloat16)
        low = (rest - mid.astype(jnp.float32)).astype(jnp.bfloat16)
        three = jnp.concatenate([hi, mid, low], axis=0)
        ex.append(jnp.exp(jnp.dot(sel_ref[...], three, preferred_element_type=jnp.float32)))
    acc_b = [None] * group
    acc_k = [None] * group
    for lv in range(levels + 1):
        if lv < levels:
            one = pair_mask(L, lv)
            mask = jnp.concatenate([one, one], axis=0)
        else:
            mask = jnp.concatenate([jnp.zeros((L, L), jnp.float32), eye], axis=0) > 0.5
        for g in range(group):
            if lv < levels:
                e0 = ex[g][2 * lv * L : (2 * lv + 1) * L]
                e1 = ex[g][(2 * lv + 1) * L : (2 * lv + 2) * L]
                left = jnp.concatenate([a[g] * e0, r[g] * e1], axis=0)
                qb, qk = b[g] * e0, k[g] * e0
            else:
                left = jnp.concatenate([a[g], r[g]], axis=0)
                qb, qk = b[g], k[g]
            sb = jnp.where(mask, mm(left, qb, (1, 1)), 0.0)
            sk = jnp.where(mask, mm(left, qk, (1, 1)), 0.0)
            acc_b[g] = sb if lv == 0 else acc_b[g] + sb
            acc_k[g] = sk if lv == 0 else acc_k[g] + sk
    inv = [eye + jnp.where(pair_mask(L, 0), acc_b[g][:L], 0.0) for g in range(group)]
    for lv in range(1, levels):
        mask = pair_mask(L, lv)
        half = [mm(inv[g], jnp.where(mask, acc_b[g][:L], 0.0)) for g in range(group)]
        inv = [inv[g] + mm(half[g], inv[g]) for g in range(group)]
    tail = 2 * levels * L
    for g in range(group):
        e_ex = ex[g][tail : tail + L]
        e_in = ex[g][tail + L : tail + 2 * L]
        e_end = ex[g][tail + 2 * L : tail + 3 * L]
        e_all = ex[g][tail + 3 * L : tail + 3 * L + size]
        w = mm(inv[g], a[g] * e_ex)
        u = mm(inv[g], mm(acc_k[g][:L], v[g]))
        b_end = b[g] * e_end
        n = base[g]
        t_buf[n] = unit_matrix(size) * e_all + mm(b_end, w, (0, 0))
        g_buf[n] = mm(b_end, u, (0, 0)) + mm(k[g] * e_end, v[g], (0, 0))
        q_buf[n] = r[g] * e_in + mm(acc_b[g][L:], w)
        o_buf[n] = mm(acc_b[g][L:], u) + mm(acc_k[g][L:], v[g])


def sigmoid(x):
    return jnp.exp(jnp.minimum(x, 0.0)) / (1.0 + jnp.exp(-jnp.abs(x)))


def halves(tile):
    size = tile.shape[1] // 2
    return tile[:, :size], pltpu.roll(tile, size, 1)[:, :size]


def layer_kernel(
    tok_ref, go_ref, gi_ref, cv_ref, rw_ref, kw_ref, vw_ref, oc_ref, os_ref, shift_ref,
    norm_ref, ddown_ref, rdown_ref, dup_ref, rup_ref, dbase_ref, rbase_ref, taps_ref, gain_ref,
    sel_ref, out_ref,
    toks, w_ref, weights, o_ref, outs, shift8_ref, shifts, ld_ref, a_ref, b_ref, k_ref, r_ref, v_ref,
    gate_ref, mixed_ref, t_buf, g_buf, q_buf, o_buf, act_ref, got_ref,
    loc_sem, zs, zr, fs_s, fs_r, ts, tr, ps, pr, hs, hr, ozs, ozr, ofs, ofr, ops, opr,
    act_s, act_r,
):
    sp, fs, tp, z, f, c = peers()
    across = [lax.rem(z + d, sp) for d in range(sp)]
    behind = [lax.rem(z + sp - d, sp) for d in range(sp)]
    beside = [lax.rem(f + d, fs) for d in range(fs)]
    other = 1 - c
    zdev = [(across[d], f, c) for d in range(sp)]
    fdev = [(z, beside[d], c) for d in range(fs)]
    partner = (z, f, other)
    rows, feats = tok_ref.shape
    orows, ocols = o_ref.shape
    wide = 2 * (go_ref.shape[1] // sp)
    size = wide // 2
    L = 64
    count = sp * rows
    nblocks = count // L

    lane = lax.broadcasted_iota(jnp.int32, (go_ref.shape[0], wide), 1)
    pairs = ((go_ref, gi_ref), (cv_ref, rw_ref), (kw_ref, vw_ref))
    for p, (first, second) in enumerate(pairs):
        for t in range(sp // 2):
            x = first[:, t * wide : (t + 1) * wide].astype(jnp.float32)
            y = second[:, t * wide : (t + 1) * wide].astype(jnp.float32)
            cols = pl.ds(p * wide, wide)
            even = jnp.where(lane < size, x, pltpu.roll(y, size, 1))
            odd = jnp.where(lane < size, pltpu.roll(x, size, 1), y)
            w_ref[2 * t, :, cols] = even.astype(jnp.bfloat16)
            w_ref[2 * t + 1, :, cols] = odd.astype(jnp.bfloat16)
    for t in range(sp):
        o_ref[2 * t * size : (2 * t + 1) * size, :] = oc_ref[t * size : (t + 1) * size, :]
        o_ref[(2 * t + 1) * size : (2 * t + 2) * size, :] = os_ref[t * size : (t + 1) * size, :]
    mixed_ref[0:8, :] = jnp.zeros((8, size), jnp.float32)
    for t in range(sp):
        shift8_ref[t] = jnp.broadcast_to(shift_ref[t], shift8_ref.shape[1:])

    line = [(lax.rem(z + d, sp), f, lax.rem(c + e, tp)) for d in range(sp) for e in range(tp)]
    greet(line[1:] + fdev[1:])
    pick = jnp.where(
        lax.broadcasted_iota(jnp.int32, (sp * size, size), 0)
        == z * size + lax.broadcasted_iota(jnp.int32, (sp * size, size), 1), 1.0, 0.0,
    ).astype(jnp.float32)

    def own_cols(ref):
        return jnp.dot(ref[...], pick, precision=HIGHEST, preferred_element_type=jnp.float32)

    def own_up(ref):
        return jnp.dot(
            ref[...], pick.astype(jnp.bfloat16), preferred_element_type=jnp.float32
        ).astype(jnp.bfloat16)

    def tok_at(zi, ci):
        return toks.at[pl.ds(pl.multiple_of(zi * rows, rows), rows),
                       pl.ds(pl.multiple_of(ci * feats, feats), feats)]

    def out_at(zi, fi, ci):
        return outs.at[pl.ds(pl.multiple_of(ci * orows, orows), orows),
                       pl.ds(pl.multiple_of((zi * fs + fi) * ocols, ocols), ocols)]

    local = [
        pltpu.make_async_copy(w_ref.at[z], weights.at[z, f], loc_sem.at[0]),
        pltpu.make_async_copy(tok_ref, tok_at(z, c), loc_sem.at[1]),
        pltpu.make_async_copy(shift8_ref.at[z], shifts.at[z], loc_sem.at[2]),
        pltpu.make_async_copy(o_ref, out_at(z, f, c), loc_sem.at[3]),
    ]
    w_z = [send(w_ref.at[across[d]], weights.at[z, f], zs.at[d], zr.at[d], zdev[d])
           for d in range(1, sp)]
    s_z = [send(shift8_ref.at[across[d]], shifts.at[z], hs.at[d], hr.at[d], zdev[d])
           for d in range(1, sp)]
    w_f = [[send(w_ref.at[z], weights.at[z, f], fs_s.at[0, e], fs_r.at[0, e], fdev[e])
            for e in range(1, fs)]]
    t_p = [send(tok_ref, tok_at(z, c), ps.at[0], pr.at[0], partner)]
    t_z = [send(tok_ref, tok_at(z, c), ts.at[d], tr.at[d], zdev[d]) for d in range(1, sp)]
    o_z = [send(o_ref, out_at(z, f, c), ozs.at[d], ozr.at[d], zdev[d]) for d in range(1, sp)]
    for copy in local:
        copy.start()
    for d in range(1, sp):
        w_z[d - 1].wait_recv()
        got = weights.at[behind[d], f]
        w_f.append([send(got, got, fs_s.at[d, e], fs_r.at[d, e], fdev[e]) for e in range(1, fs)])
    o_f = [send(o_ref, out_at(z, f, c), ofs.at[0, e], ofr.at[0, e], fdev[e])
           for e in range(1, fs)]
    o_p = [send(o_ref, out_at(z, f, c), ops.at[0, 0], opr.at[0, 0], partner)]
    for d in range(1, sp):
        t_z[d - 1].wait_recv()
        got = tok_at(behind[d], c)
        t_p.append(send(got, got, ps.at[d], pr.at[d], partner))
    for copy in local:
        copy.wait()
    for copies in w_f:
        for copy in copies:
            copy.wait_recv()

    def pass_out(d):
        o_z[d - 1].wait_recv()
        got = out_at(behind[d], f, c)
        o_p.append(send(got, got, ops.at[d, 0], opr.at[d, 0], partner))
        o_f.extend(send(got, got, ofs.at[d, e], ofr.at[d, e], fdev[e]) for e in range(1, fs))

    dup, rup = own_up(dup_ref), own_up(rup_ref)
    dbase, rbase, gain = own_cols(dbase_ref), own_cols(rbase_ref), own_cols(gain_ref)
    taps = own_cols(taps_ref)
    low_w = jnp.concatenate([ddown_ref[...], rdown_ref[...]], axis=0)
    all_w = weights[...].reshape(sp * fs * w_ref.shape[1], w_ref.shape[2])
    for d in range(sp):
        t_p[d].wait_recv()
        if d:
            s_z[d - 1].wait_recv()
        start = pl.multiple_of(behind[d] * rows, rows)
        here = pl.ds(start, rows)
        x = toks[here, :].astype(jnp.float32)
        normed = (
            x * lax.rsqrt(jnp.mean(x * x, axis=-1, keepdims=True) + RMS_EPS) * norm_ref[...]
        ).astype(jnp.bfloat16)
        proj = jnp.dot(normed, all_w, preferred_element_type=jnp.float32)
        proj = proj.astype(jnp.bfloat16).astype(jnp.float32)
        lows = lax.dot_general(
            normed, low_w, (((1,), (1,)), ((), ())), preferred_element_type=jnp.float32
        )
        decay_low, rate_low = halves(lows)
        decay_sig = sigmoid(dbase + jnp.dot(
            jnp.tanh(decay_low).astype(jnp.bfloat16), dup, preferred_element_type=jnp.float32
        ))
        rate = sigmoid(rbase + jnp.dot(
            rate_low.astype(jnp.bfloat16), rup, preferred_element_type=jnp.float32
        ))
        gate_out, gate_in = halves(proj[:, :wide])
        conv_in, recv = halves(proj[:, wide : 2 * wide])
        keys, vals = halves(proj[:, 2 * wide :])
        column = jnp.transpose(shifts[behind[d]])[:, 0:1]
        ld_ref[here, :] = -decay_sig * jnp.exp(column - 0.5)
        unit = keys * lax.rsqrt(jnp.sum(keys * keys, axis=-1, keepdims=True) + UNIT_EPS)
        a_ref[here, :] = -unit
        b_ref[here, :] = unit * rate
        k_ref[here, :] = keys * rate
        r_ref[here, :] = recv
        v_ref[here, :] = vals
        gate_ref[here, :] = gate_out
        mixed_ref[pl.ds(pl.multiple_of(start + 8, 8), rows), :] = gate_in * conv_in

    fields = (ld_ref, a_ref, b_ref, k_ref, r_ref, v_ref)
    bufs = (t_buf, g_buf, q_buf, o_buf)
    group = 2
    trips = nblocks // group
    cuts = [trips * i // sp for i in range(sp + 1)]
    for i in range(sp):
        def several(n, _):
            blocks_of(n * group, group, L, fields, sel_ref, bufs)
            return 0

        lax.fori_loop(cuts[i], cuts[i + 1], several, 0)
        if i:
            pass_out(i)

    me = z * tp + c
    mine = got_ref.at[:, pl.ds(pl.multiple_of((c * sp + z) * wide, wide), wide)]

    def act_copy(n):
        return pltpu.make_async_remote_copy(
            src_ref=act_ref.at[n], dst_ref=mine, send_sem=act_s.at[n], recv_sem=act_r.at[me],
            device_id=(n // tp, f, n % tp), device_id_type=MESH,
        )

    def own_copy(n):
        return pltpu.make_async_copy(act_ref.at[n], mine, act_s.at[n])

    def give(n):
        @pl.when(me != n)
        def _():
            act_copy(n).start()

        @pl.when(me == n)
        def _():
            own_copy(n).start()

    state = jnp.zeros((size, size), jnp.float32)
    for n in range(nblocks):
        read = mm(q_buf[n], state) + o_buf[n]
        state = mm(t_buf[n], state) + g_buf[n]
        centred = read - jnp.mean(read, axis=-1, keepdims=True)
        variance = jnp.mean(centred * centred, axis=-1, keepdims=True)
        done = centred * lax.rsqrt(variance + GROUP_EPS) * gain
        spot = n * L + 8
        convolved = (
            mixed_ref[spot - 2 : spot - 2 + L, :] * taps[0:1]
            + mixed_ref[spot - 1 : spot - 1 + L, :] * taps[1:2]
            + mixed_ref[spot : spot + L, :] * taps[2:3]
        )
        conv = gate_ref[n * L : (n + 1) * L, :] * convolved
        act_ref[n] = jnp.concatenate([conv, done], axis=1).astype(jnp.bfloat16)
        if n:
            give(n - 1)
    for d in range(sp):
        for e in range(1, fs):
            o_f[d * (fs - 1) + e - 1].wait_recv()
            got = out_at(behind[d], lax.rem(f + fs - e, fs), c)
            o_p.append(send(got, got, ops.at[d, e], opr.at[d, e], partner))
        if d == 0:
            give(nblocks - 1)
    for n in range(nblocks):
        @pl.when(me != n)
        def _():
            act_copy(n).wait_send()
            pltpu.make_async_remote_copy(
                src_ref=act_ref.at[n],
                dst_ref=got_ref.at[:, pl.ds(((n % tp) * sp + n // tp) * wide, wide)],
                send_sem=act_s.at[n], recv_sem=act_r.at[n],
                device_id=partner, device_id_type=MESH,
            ).wait_recv()

        @pl.when(me == n)
        def _():
            own_copy(n).wait()
    for copy in o_p:
        copy.wait()
    step = 512

    def columns(i, _):
        cols = pl.ds(pl.multiple_of(i * step, step), step)
        out_ref[:, cols] = jnp.dot(
            got_ref[...], outs[:, cols], preferred_element_type=jnp.float32
        ).astype(out_ref.dtype)
        return 0

    lax.fori_loop(0, outs.shape[1] // step, columns, 0)
    for copy in w_z + t_z + o_z + o_f + s_z:
        copy.wait_send()
    for copies in w_f:
        for copy in copies:
            copy.wait_send()
    for copy in t_p:
        copy.wait_send()


def head_body(
    tokens, norm_gain, conv_gate_out, conv_gate_in, conv_value, conv_taps, recv_weight,
    key_weight, value_weight, decay_base, decay_down, decay_up, decay_shift, rate_base,
    rate_down, rate_up, head_gain, out_conv, out_state,
):
    sp, fs, tp = (lax.axis_size(name) for name in ("sp", "fs", "tp"))
    rows = tokens.shape[1]
    size = recv_weight.shape[1] // sp
    own_rows = conv_gate_out.shape[0]
    tok = tokens.reshape(rows, tokens.shape[2])
    shift = decay_shift.reshape(rows, sp).T.reshape(sp, 1, rows)
    length = 64
    count = sp * rows
    nblocks = count // length
    sel = jnp.asarray(range_rows(length), jnp.bfloat16)
    vm = pl.BlockSpec(memory_space=pltpu.VMEM)
    dma = pltpu.SemaphoreType.DMA
    o_rows, o_cols = 2 * out_conv.shape[0], out_conv.shape[1]
    model = out_conv.shape[1] * sp * fs
    f32, bf16 = jnp.float32, jnp.bfloat16
    field = pltpu.VMEM((count, size), f32)
    block = pltpu.VMEM((nblocks, length, size), f32)
    mixed = pl.pallas_call(
        layer_kernel,
        out_shape=jax.ShapeDtypeStruct((count // (sp * tp), model), bf16),
        in_specs=[vm] * 20,
        out_specs=vm,
        scratch_shapes=[
            pltpu.VMEM((count, tp * tok.shape[1]), bf16),
            pltpu.VMEM((sp, own_rows, 6 * size), bf16),
            pltpu.VMEM((sp, fs, own_rows, 6 * size), bf16),
            pltpu.VMEM((o_rows, o_cols), bf16),
            pltpu.VMEM((tp * o_rows, model), bf16),
            pltpu.VMEM((sp, 8, rows), f32),
            pltpu.VMEM((sp, 8, rows), f32),
            field, field, field, field, field, field, field,
            pltpu.VMEM((count + 8, size), f32),
            block, block, block, block,
            pltpu.VMEM((nblocks, length, 2 * size), bf16),
            pltpu.VMEM((length, tp * o_rows), bf16),
            dma((4,)), dma((sp,)), dma((sp,)), dma((sp, fs)), dma((sp, fs)), dma((sp,)), dma((sp,)),
            dma((sp,)), dma((sp,)), dma((sp,)), dma((sp,)), dma((sp,)), dma((sp,)),
            dma((sp, fs)), dma((sp, fs)), dma((sp, fs)), dma((sp, fs)),
            dma((nblocks,)), dma((nblocks,)),
        ],
        compiler_params=pltpu.CompilerParams(
            collective_id=0, has_side_effects=True, vmem_limit_bytes=56 * 1024 * 1024
        ),
    )(
        tok, conv_gate_out, conv_gate_in, conv_value, recv_weight, key_weight, value_weight,
        out_conv, out_state, shift, norm_gain.reshape(1, -1), decay_down.T, rate_down.T, decay_up,
        rate_up, decay_base.reshape(1, -1), rate_base.reshape(1, -1), conv_taps,
        head_gain.reshape(1, -1), sel,
    )
    return mixed.reshape((1,) + mixed.shape)


def one_head_each(mesh, tokens, shift, weight):
    sp, tp = mesh.shape["sp"], mesh.shape["tp"]
    heads = shift.shape[2]
    count = tokens.shape[1] // sp
    size = weight.shape[1] // heads
    return (
        tp == 2
        and heads == sp * tp
        and tokens.shape[0] == mesh.shape["fs"]
        and size == 64
        and count == tp * 64
        and sp % 2 == 0
        and weight.shape[0] % (sp * mesh.shape["fs"] * 16) == 0
    )


def solution(mesh):
    placed = (
        P("fs", "sp", "tp"),
        P(),
        P(("sp", "fs"), "tp"),
        P(("sp", "fs"), "tp"),
        P(("sp", "fs"), "tp"),
        P(None, "tp"),
        P(("sp", "fs"), "tp"),
        P(("sp", "fs"), "tp"),
        P(("sp", "fs"), "tp"),
        P("tp"),
        P(),
        P(None, "tp"),
        P("fs", "sp", "tp"),
        P("tp"),
        P(),
        P(None, "tp"),
        P("tp"),
        P("tp", ("sp", "fs")),
        P("tp", ("sp", "fs")),
    )
    def run(*args):
        chosen = head_body if one_head_each(mesh, args[0], args[12], args[6]) else body
        return jax.shard_map(
            chosen, mesh=mesh, in_specs=placed, out_specs=P("fs", ("sp", "tp"), None),
            check_vma=False,
        )(*args)

    return run
```
